32 devices in a mesh: gr: 2 (over y), fs: 4 (over z), tp: 4 (over x, core).
Axes of the slice: x: 2, y: 2, z: 4, core: 2. Of those that a mesh axis runs over, the one named last changes fastest.
Arguments:
- tokens: bfloat16 [4096, 2048], P(('gr', 'tp'), 'fs'), may hold values from -6 to 6
- routes: int32 [4096, 2], P(('gr', 'tp')), may hold values from 0 to 7, all different within a row; in each aligned block of 512 rows (0 to 511, 512 to 1023, ...) at most 192 rows name the same one
- route_weight: float32 [4096, 2], P(('gr', 'tp')), may hold values from 0.25 to 1
- norm_gain: float32 [2048], P(('gr', 'fs')), may hold values from 0.1 to 1.9
- gate_master: float32 [8, 2048, 2816], P(None, ('gr', 'fs'), 'tp'), may hold values from -0.125 to 0.125
- up_master: float32 [8, 2048, 2816], P(None, ('gr', 'fs'), 'tp'), may hold values from -0.125 to 0.125
- down_master: float32 [8, 2048, 2816], P(None, ('gr', 'fs'), 'tp'), may hold values from -0.109375 to 0.109375
Outputs:
- mixed_output: bfloat16 [4096, 2048], P(('gr', 'tp'), 'fs')
- gate_serving: bfloat16 [8, 2048, 2816], P('tp', None, 'fs')
- up_serving: bfloat16 [8, 2048, 2816], P('tp', None, 'fs')
- down_serving: bfloat16 [8, 2048, 2816], P('tp', None, 'fs')
The draws below stay inside these ranges and needn't reach their ends.
Inputs may be any that keep to these rules, and one draw needn't show every extreme that they name: `routes`: each row names two different experts. Within the rows of one block of 512 tokens (one index of gr+tp) no expert is named by more than 192 rows, and in some blocks one expert is named by exactly 192.
All inputs are finite; a program needn't handle non-finite values.
Results may differ from the reference program's by a relative error of at most 0.0082.
Values may be sent and summed in bfloat16 or wider, within the bound.
A program may use at most 128 MiB of HBM per device.

```python
import math
import jax
import jax.numpy as jnp
import numpy as np
from jax import lax

D = 2048
EFF = 2816
EXPERTS = 8
TOK_DEV = 512
CAP = 192
TOKENS = 4096


def shard_levels(stream_key, dims, cuts, low, largest):
    loudness, own = 1.0, jax.random.fold_in(stream_key, 6)
    for dim, blocks in cuts:
        steps = jnp.exp(jax.random.uniform(jax.random.fold_in(own, dim), (blocks,), jnp.float32, low / len(cuts), largest / len(cuts)))
        loudness = loudness * jnp.repeat(steps, dims[dim] // blocks).reshape([-1 if axis == dim else 1 for axis in range(len(dims))])
    return loudness


def deal_out(stream_key, own, number, rows, count, top, bound, skew):
    ranking = jax.random.permutation(stream_key, count)
    heavy_load, common = portions_of(count, rows * top, bound, skew, True), portions_of(count, rows * top, bound, skew, False)
    places = jnp.arange(count)

    def named(tallies, rotation):
        used = int((tallies > 0).sum())
        fixed = max(1, used // 4)
        passed = fixed + (places - fixed + rotation * (used - fixed)) % max(1, count - fixed)
        return jnp.zeros((count,), jnp.int32).at[ranking[jnp.where(places < fixed, places, passed)]].set(jnp.asarray(tallies, jnp.int32))

    tallies = jnp.where(number % 4 == 0, named(heavy_load, number // 4), named(common, number - number // 4 - 1))
    mixed = jax.random.permutation(jax.random.fold_in(own, 3), count)
    source_of, sink = mixed[0:count // 2 * 2:2], mixed[1:count // 2 * 2:2]
    slack = jnp.minimum(tallies[source_of] - 1, bound - tallies[sink]) // 2
    slack = jnp.where((source_of == ranking[0]) | (sink == ranking[0]) | (tallies[sink] == 0), 0, jnp.maximum(slack, 0))
    passed = jax.random.randint(jax.random.fold_in(own, 4), (count // 2,), 0, 1 << 20) % (slack + 1)
    tallies = tallies.at[source_of].add(-passed).at[sink].add(passed)
    members = jnp.searchsorted(jnp.cumsum(tallies), jnp.arange(rows * top), side="right").astype(jnp.int32)
    grid = members.reshape(top, rows).T
    grid = grid[jax.random.permutation(jax.random.fold_in(own, 1), rows)]
    rotation = jax.random.randint(jax.random.fold_in(own, 2), (rows, 1), 0, top)
    return jnp.take_along_axis(grid, (jnp.arange(top)[None, :] + rotation) % top, axis=1)


def portions_of(count, total, reach, slope, full):
    portions = [(1 << 20) // math.isqrt(standing ** slope) + 1 for standing in range(1, count + 1)]
    largest = reach if full else min(reach, max(-(-total // count), total * portions[0] // sum(portions)))
    least = 1 if total - largest >= count - 1 else 0
    holding, rest = [largest] + [least] * (count - 1), total - largest - least * (count - 1)
    while rest > 0:
        candidates = [i for i in range(1, count) if holding[i] < largest] or [i for i in range(1, count) if holding[i] < reach]
        whole, left = sum([portions[i] for i in candidates]), rest
        for i in candidates:
            addition = min(reach - holding[i], max(1, left * portions[i] // whole), rest)
            holding[i] = holding[i] + addition
            rest = rest - addition
    return np.array(holding)


def normal_values(key, shape, deviation, bound, cuts=(), held_as=jnp.bfloat16):
    values = deviation * jax.random.normal(key, shape, jnp.float32)
    if cuts:
        values = values * shard_levels(key, shape, cuts, -0.22, 0.18)
    return jnp.clip(values, -bound, bound).astype(held_as)


def setup_inputs(seed: int = 0) -> dict:
    arg_keys = jax.random.split(jax.random.key(seed), 8)
    tokens = normal_values(arg_keys[0], (TOKENS, D), 1.0, 6.0, ((0, 8), (1, 4)))
    routes_keys = jax.random.split(jax.random.fold_in(arg_keys[1], 1), TOKENS // TOK_DEV)
    routes_turns = jax.random.permutation(jax.random.fold_in(arg_keys[1], 3), TOKENS // TOK_DEV)
    routes = jax.vmap(lambda own, number: deal_out(jax.random.fold_in(arg_keys[1], 2), own, number, TOK_DEV, EXPERTS, 2, CAP, 1))(routes_keys, routes_turns).reshape((TOKENS, 2))
    route_weight = jnp.clip(jnp.exp(math.log(1.0) - 1.3862944 * jax.random.uniform(arg_keys[2], (TOKENS, 2), jnp.float32) ** shard_levels(arg_keys[2], (TOKENS, 2), ((0, 8),), -0.2, 0.2)), 0.25, 1.0)
    norm_gain = jnp.clip(1.0 + 0.18 * jax.random.normal(arg_keys[3], (D,), jnp.float32), 0.1, 1.9)
    gate_master = normal_values(arg_keys[4], (EXPERTS, D, EFF), D ** -0.5, 0.125, ((1, 8), (2, 4)), jnp.float32)
    up_master = normal_values(arg_keys[5], (EXPERTS, D, EFF), D ** -0.5, 0.125, ((1, 8), (2, 4)), jnp.float32)
    down_master = normal_values(arg_keys[6], (EXPERTS, D, EFF), EFF ** -0.5, 0.109375, ((1, 8), (2, 4)), jnp.float32)
    return {"tokens": tokens, "routes": routes, "route_weight": route_weight, "norm_gain": norm_gain, "gate_master": gate_master, "up_master": up_master, "down_master": down_master}


norm_eps = 1e-06

def slot_table(routes, experts, capacity):
    flat_routes = routes.reshape(-1)
    onehot = (flat_routes[:, None] == jnp.arange(experts, dtype=jnp.int32)[None, :]).astype(jnp.int32)
    running = jnp.cumsum(onehot, axis=0)
    slot_index = lax.optimization_barrier(jnp.sum(onehot * (running - 1), axis=1))
    return (flat_routes * capacity + slot_index).astype(jnp.int32)

def reference(tokens, routes, route_weight, norm_gain, gate_master, up_master, down_master):
    gate_serving = (gate_master * norm_gain[None, :, None]).astype(jnp.bfloat16)
    up_serving = (up_master * norm_gain[None, :, None]).astype(jnp.bfloat16)
    down_serving = down_master.astype(jnp.bfloat16)
    blocks = TOKENS // TOK_DEV
    as_float = tokens.astype(jnp.float32)
    normed = (as_float * lax.rsqrt(lax.optimization_barrier(jnp.mean(as_float * as_float, axis=1, keepdims=True)) + norm_eps)).astype(jnp.bfloat16)
    normed = normed.reshape(blocks, TOK_DEV, D)
    route_blocks = routes.reshape(blocks, TOK_DEV, 2)

    def find_slots(block_routes):
        return slot_table(block_routes, EXPERTS, CAP)
    placing = jax.vmap(find_slots)(route_blocks)
    slot_rows = jnp.arange(EXPERTS * CAP, dtype=jnp.int32)

    def pick(block_places):
        return (slot_rows[:, None] == block_places[None, :]).reshape(EXPERTS * CAP, TOK_DEV, 2)

    def dispatch(block_places, block_rows):
        route_table = lax.optimization_barrier(jnp.sum(pick(block_places).astype(jnp.float32), axis=2)).astype(jnp.bfloat16)
        return jnp.dot(route_table, block_rows, preferred_element_type=jnp.float32).astype(jnp.bfloat16)
    outgoing = jax.vmap(dispatch)(placing, normed)
    outgoing = outgoing.reshape(blocks, EXPERTS, CAP, D).transpose(1, 0, 2, 3).reshape(EXPERTS, blocks * CAP, D)

    def expert(inputs):
        slots, w_gate, w_up, w_down = inputs
        gate_acc = jnp.dot(slots, w_gate, preferred_element_type=jnp.float32)
        up_acc = jnp.dot(slots, w_up, preferred_element_type=jnp.float32)
        hidden = (jax.nn.silu(gate_acc) * up_acc).astype(jnp.bfloat16)
        return lax.dot_general(hidden, w_down, (((1,), (1,)), ((), ())), preferred_element_type=jnp.float32)
    outputs = lax.map(expert, (outgoing, gate_serving, up_serving, down_serving))
    outputs = outputs.reshape(EXPERTS, blocks, CAP, D).transpose(1, 0, 2, 3).reshape(blocks, EXPERTS * CAP, D)

    def combine(block_places, weight, produced):
        weights = lax.optimization_barrier(jnp.sum(jnp.where(pick(block_places), weight.reshape(1, TOK_DEV, 2), 0.0), axis=2))
        return lax.dot_general(weights, produced, (((0,), (0,)), ((), ())), precision=lax.Precision.HIGHEST, preferred_element_type=jnp.float32)
    mixed_output = jax.vmap(combine)(placing, route_weight.reshape(blocks, TOK_DEV, 2), outputs)
    return (mixed_output.reshape(TOKENS, D).astype(jnp.bfloat16), gate_serving, up_serving, down_serving)
```

```python
import functools

import jax
import jax.numpy as jnp
from jax import lax
from jax.experimental import pallas as pl
from jax.experimental.pallas import tpu as pltpu
from jax.sharding import PartitionSpec as P

norm_eps = 1e-06
MESH = pl.DeviceIdType.MESH


def slot_table(routes, experts, capacity):
    flat_routes = routes.reshape(-1)
    onehot = (flat_routes[:, None] == jnp.arange(experts, dtype=jnp.int32)[None, :]).astype(
        jnp.int32
    )
    running = jnp.cumsum(onehot, axis=0)
    slot_index = jnp.sum(onehot * (running - 1), axis=1)
    return flat_routes * capacity + slot_index


def spread_kernel(sizes, count, flipped, *refs):
    gr, fs, tp, sub, local_experts, rows = sizes
    ins, outs, relays = refs[:count], refs[count : 2 * count], refs[2 * count : 3 * count]
    bounce, tp_send, tp_recv, fs_send, fs_recv, gr_send, gr_recv, load_sem, store_sem = refs[
        3 * count :
    ]
    g, f, t = lax.axis_index("gr"), lax.axis_index("fs"), lax.axis_index("tp")
    blocks = [(w, j) for j in range(local_experts) for w in range(count)]

    barrier = pltpu.get_barrier_semaphore()
    for axis, me, size in (("gr", g, gr), ("fs", f, fs), ("tp", t, tp)):
        for d in range(1, size):
            pl.semaphore_signal(
                barrier, inc=1, device_id={axis: lax.rem(me + d, size)}, device_id_type=MESH
            )
    pl.semaphore_wait(barrier, gr + fs + tp - 3)

    def out_rows(c, group, source):
        w, j = blocks[c]
        start = pl.multiple_of((group * fs + source) * rows, rows)
        if flipped:
            return outs[w].at[j, :, pl.ds(start, rows)]
        return outs[w].at[j, pl.ds(start, rows)]

    def own(c, target, s):
        w, j = blocks[c]
        return ins[w].at[s, target * local_experts + j]

    def relay(c, source, s):
        w, j = blocks[c]
        return relays[w].at[j, source, s]

    def tp_copy(c, d, s, to_out):
        target = lax.rem(t + d, tp)
        return pltpu.make_async_remote_copy(
            src_ref=own(c, target, s),
            dst_ref=out_rows(c, g, f) if to_out else relay(c, t, s),
            send_sem=tp_send.at[c, d, s],
            recv_sem=tp_recv.at[c, d, s],
            device_id={"tp": target},
            device_id_type=MESH,
        )

    def fs_copy(c, d, s, src, target):
        return pltpu.make_async_remote_copy(
            src_ref=src,
            dst_ref=out_rows(c, g, f),
            send_sem=fs_send.at[c, d, s],
            recv_sem=fs_recv.at[c, f],
            device_id={"fs": target},
            device_id_type=MESH,
        )

    def gr_copy(c, n, source, src):
        return pltpu.make_async_remote_copy(
            src_ref=src,
            dst_ref=out_rows(c, g, source),
            send_sem=gr_send.at[c, n, source],
            recv_sem=gr_recv.at[c, n, source],
            device_id={"gr": lax.rem(g + n, gr)},
            device_id_type=MESH,
        )

    def to_groups(c, source, src):
        for n in range(1, gr):
            gr_copy(c, n, source, src).start()

    def tp_start(c):
        for d in range(1, tp):
            for s in range(sub):

                @pl.when(t * sub + s == f)
                def _():
                    tp_copy(c, d, s, True).start()

                @pl.when(t * sub + s != f)
                def _():
                    tp_copy(c, d, s, False).start()

    def own_start(c):
        for s in range(sub):
            target = t * sub + s

            @pl.when(target != f)
            def _():
                fs_copy(c, 0, s, own(c, t, s), target).start()

            @pl.when(target == f)
            def _():
                pltpu.make_async_copy(own(c, t, s), bounce.at[c], load_sem.at[c]).start()
                to_groups(c, f, own(c, t, s))

    def own_store(c):
        for s in range(sub):

            @pl.when(t * sub + s == f)
            def _():
                pltpu.make_async_copy(own(c, t, s), bounce.at[c], load_sem.at[c]).wait()
                pltpu.make_async_copy(bounce.at[c], out_rows(c, g, f), store_sem.at[c]).start()

    def tp_arrived(c):
        for d in range(1, tp):
            source = lax.rem(t + tp - d, tp)
            for s in range(sub):
                target = source * sub + s

                @pl.when(target == f)
                def _():
                    tp_copy(c, d, s, True).wait_recv()
                    to_groups(c, f, out_rows(c, g, f))

                @pl.when(target != f)
                def _():
                    pltpu.make_async_remote_copy(
                        src_ref=own(c, t, s),
                        dst_ref=relay(c, source, s),
                        send_sem=tp_send.at[c, d, s],
                        recv_sem=tp_recv.at[c, d, s],
                        device_id={"tp": source},
                        device_id_type=MESH,
                    ).wait_recv()
                    fs_copy(c, d, s, relay(c, source, s), target).start()

    def fs_arrived(c):
        for d in range(1, fs):
            source = lax.rem(f + d, fs)
            pltpu.make_async_remote_copy(
                src_ref=own(c, t, 0),
                dst_ref=out_rows(c, g, source),
                send_sem=fs_send.at[c, 0, 0],
                recv_sem=fs_recv.at[c, source],
                device_id={"fs": source},
                device_id_type=MESH,
            ).wait_recv()
            to_groups(c, source, out_rows(c, g, source))

    total = len(blocks)
    ahead = min(3, total)
    own_start(0)
    for c in range(ahead):
        tp_start(c)
    for c in range(total + 1):
        if c + ahead < total:
            tp_start(c + ahead)
        if c + 1 < total:
            own_start(c + 1)
        if c < total:
            own_store(c)
            tp_arrived(c)
        if c >= 1:
            fs_arrived(c - 1)

    for c in range(total):
        for n in range(1, gr):
            for source in range(fs):
                group = lax.rem(g + gr - n, gr)
                pltpu.make_async_remote_copy(
                    src_ref=own(c, t, 0),
                    dst_ref=out_rows(c, group, source),
                    send_sem=gr_send.at[c, n, source],
                    recv_sem=gr_recv.at[c, n, source],
                    device_id={"gr": group},
                    device_id_type=MESH,
                ).wait_recv()
                gr_copy(c, n, source, out_rows(c, g, source)).wait_send()
        for s in range(sub):
            for d in range(1, tp):
                tp_copy(c, d, s, False).wait_send()
            for d in range(tp):
                target = lax.rem(t + tp - d, tp) * sub + s

                @pl.when(target != f)
                def _():
                    fs_copy(c, d, s, own(c, t, s), target).wait_send()

            @pl.when(t * sub + s == f)
            def _():
                pltpu.make_async_copy(bounce.at[c], out_rows(c, g, f), store_sem.at[c]).wait()


def spread(*weights):
    gr, fs, tp = lax.axis_size("gr"), lax.axis_size("fs"), lax.axis_size("tp")
    experts, rows, columns = weights[0].shape
    local_experts = experts // tp
    assert fs % tp == 0
    sub = fs // tp
    width = columns // sub
    count = len(weights)
    total = count * local_experts
    flipped = rows % 128 == 0
    order = (2, 0, 3, 1) if flipped else (2, 0, 1, 3)
    parts = [w.reshape(experts, rows, sub, width).transpose(order) for w in weights]
    block = (width, rows) if flipped else (rows, width)
    whole = (width, gr * fs * rows) if flipped else (gr * fs * rows, width)
    served = jax.ShapeDtypeStruct((local_experts, *whole), jnp.bfloat16)
    relayed = jax.ShapeDtypeStruct((local_experts, tp, sub, *block), jnp.bfloat16)
    dma = pltpu.SemaphoreType.DMA
    sent = 2 * total * rows * columns * (tp - 1 + fs - 1 + (gr - 1) * fs) // fs
    found = pl.pallas_call(
        functools.partial(spread_kernel, (gr, fs, tp, sub, local_experts, rows), count, flipped),
        out_shape=[served] * count + [relayed] * count,
        in_specs=[pl.BlockSpec(memory_space=pl.ANY)] * count,
        out_specs=[pl.BlockSpec(memory_space=pl.ANY)] * (2 * count),
        scratch_shapes=[
            pltpu.VMEM((total, *block), jnp.bfloat16),
            dma((total, tp, sub)),
            dma((total, tp, sub)),
            dma((total, tp, sub)),
            dma((total, fs)),
            dma((total, gr, fs)),
            dma((total, gr, fs)),
            dma((total,)),
            dma((total,)),
        ],
        compiler_params=pltpu.CompilerParams(collective_id=0, has_side_effects=True),
        cost_estimate=pl.CostEstimate(flops=0, bytes_accessed=40 * sent, transcendentals=0),
    )(*parts)
    return [w.swapaxes(1, 2) if flipped else w for w in found[:count]]


def local_by_collectives(tokens, routes, route_weight, norm_gain, gate_master, up_master, down_master):
    experts = gate_master.shape[0]
    tp_count = lax.axis_size("tp")
    fs_count = lax.axis_size("fs")
    local_experts = experts // tp_count
    token_rows = tokens.shape[0]
    model_width = tokens.shape[1] * fs_count
    capacity = 3 * token_rows // experts
    scaled_gain = norm_gain[None, :, None]
    gate_w = (gate_master * scaled_gain).astype(jnp.bfloat16)
    up_w = (up_master * scaled_gain).astype(jnp.bfloat16)
    down_w = down_master.astype(jnp.bfloat16)
    gate_w, up_w, down_w = spread(gate_w, up_w, down_w)
    as_float = tokens.astype(jnp.float32)
    square_total = lax.psum(jnp.sum(as_float * as_float, axis=1), "fs")
    normed = (as_float * lax.rsqrt(square_total / model_width + norm_eps)[:, None]).astype(
        jnp.bfloat16
    )
    placing = slot_table(routes, experts, capacity)
    slot_rows = jnp.arange(experts * capacity, dtype=jnp.int32)
    picked = (slot_rows[:, None] == placing[None, :]).reshape(experts * capacity, token_rows, 2)
    route_table = jnp.sum(picked.astype(jnp.float32), axis=2).astype(jnp.bfloat16)
    outgoing = jnp.dot(route_table, normed, preferred_element_type=jnp.float32).astype(jnp.bfloat16)
    outgoing = outgoing.reshape(tp_count, local_experts, capacity, tokens.shape[1])
    shard_piece = lax.all_gather(
        lax.all_to_all(outgoing, "tp", split_axis=0, concat_axis=0, tiled=True),
        "fs",
        axis=3,
        tiled=True,
    )
    returned = []
    for j in range(local_experts):
        rows = shard_piece[:, j]
        gate_acc = jnp.einsum("scd,df->scf", rows, gate_w[j], preferred_element_type=jnp.float32)
        up_acc = jnp.einsum("scd,df->scf", rows, up_w[j], preferred_element_type=jnp.float32)
        hidden = (jax.nn.silu(gate_acc) * up_acc).astype(jnp.bfloat16)
        partial_value = jnp.einsum(
            "scf,df->scd", hidden, down_w[j], preferred_element_type=jnp.float32
        )
        summed = lax.psum_scatter(
            partial_value.astype(jnp.bfloat16), "fs", scatter_dimension=2, tiled=True
        )
        returned.append(lax.all_to_all(summed, "tp", split_axis=0, concat_axis=0, tiled=True))
    produced = jnp.stack(returned, axis=1)
    produced = produced.reshape(experts * capacity, produced.shape[3])
    pair_slots = placing.reshape(token_rows, 2)
    first_rows = jnp.take(produced, pair_slots[:, 0], axis=0)
    second_rows = jnp.take(produced, pair_slots[:, 1], axis=0)
    mixed_out = first_rows * route_weight[:, 0:1] + second_rows * route_weight[:, 1:2]
    return (mixed_out.astype(jnp.bfloat16), gate_w, up_w, down_w)


def slot_places(routes, experts, capacity):
    rows = routes.shape[0]
    hits = (routes[:, :, None] == jnp.arange(experts, dtype=jnp.int32)).astype(jnp.int32)
    both = hits[:, 0] + hits[:, 1]
    before = jnp.cumsum(both, axis=0) - both
    first = jnp.sum(hits[:, 0] * before, axis=1)
    second = jnp.sum(hits[:, 1] * (before + hits[:, 0]), axis=1)
    places = jnp.stack([first, second]) + routes.T * capacity
    return jnp.pad(places, ((0, 6), (0, 0)))


def serve_kernel(sizes, *refs):
    gr, fs, tp, local_experts, rows, capacity = sizes
    tokens, places, shares = refs[:3]
    ins, outs, relays, partial = refs[3:6], refs[6:9], refs[9:12], refs[12]
    (
        bounce, gathered, place_of, share_of, picks, slot_share, slots, hid, spread_hid,
        gate_buf, up_buf, down_buf, part_buf,
        tp_send, tp_recv, fs_send, fs_recv, gr_send, gr_recv, load_sem, store_sem,
        tokz_send, tokz_recv, tokt_send, tokt_recv, info_send, info_recv, own_sem,
        weight_sem, down_sem, part_sem,
    ) = refs[13:]
    count = 3
    g, f, t = lax.axis_index("gr"), lax.axis_index("fs"), lax.axis_index("tp")
    blocks = [(w, j) for j in range(local_experts) for w in range(2)]
    blocks += [(2, j) for j in range(local_experts)]
    total = len(blocks)
    token_rows, features = tokens.shape
    width = gathered.shape[2]

    barrier = pltpu.get_barrier_semaphore()
    for axis, me, size in (("gr", g, gr), ("fs", f, fs), ("tp", t, tp)):
        for d in range(1, size):
            pl.semaphore_signal(
                barrier, inc=1, device_id={axis: lax.rem(me + d, size)}, device_id_type=MESH
            )
    pl.semaphore_wait(barrier, gr + fs + tp - 3)

    def remote(src, dst, send, recv, axis, target):
        return pltpu.make_async_remote_copy(
            src_ref=src, dst_ref=dst, send_sem=send, recv_sem=recv,
            device_id={axis: target}, device_id_type=MESH,
        )

    def slab(block, source):
        start = pl.multiple_of(source * features, features)
        return gathered.at[block, :, pl.ds(start, features)]

    def tokz(d):
        return remote(
            tokens, slab(t, f), tokz_send.at[d], tokz_recv.at[f], "fs", lax.rem(f + d, fs)
        )

    def tokz_from(d):
        source = lax.rem(f + fs - d, fs)
        return source, remote(
            tokens, slab(t, source), tokz_send.at[d], tokz_recv.at[source], "fs", source
        )

    def tokt(d, source):
        return remote(
            slab(t, source), slab(t, source), tokt_send.at[d, source], tokt_recv.at[t, source],
            "tp", lax.rem(t + d, tp),
        )

    def info(d, k):
        whole = (place_of, share_of)[k]
        return remote(
            (places, shares)[k], whole.at[t], info_send.at[d, k], info_recv.at[t, k],
            "tp", lax.rem(t + d, tp),
        )

    def own_copies():
        return (
            pltpu.make_async_copy(tokens, slab(t, f), own_sem.at[0]),
            pltpu.make_async_copy(places, place_of.at[t], own_sem.at[1]),
            pltpu.make_async_copy(shares, share_of.at[t], own_sem.at[2]),
        )

    def out_rows(c, group, source):
        w, j = blocks[c]
        start = pl.multiple_of((group * fs + source) * rows, rows)
        return outs[w].at[j, :, pl.ds(start, rows)]

    def own(c, target):
        w, j = blocks[c]
        return ins[w].at[target * local_experts + j]

    def relay(c, source):
        w, j = blocks[c]
        return relays[w].at[j, source]

    def tp_copy(c, d, to_out):
        target = lax.rem(t + d, tp)
        return remote(
            own(c, target), out_rows(c, g, f) if to_out else relay(c, t),
            tp_send.at[c, d], tp_recv.at[c, d], "tp", target,
        )

    def fs_copy(c, d, src, target):
        return remote(src, out_rows(c, g, f), fs_send.at[c, d], fs_recv.at[c, f], "fs", target)

    def gr_copy(c, n, source, src):
        return remote(
            src, out_rows(c, g, source), gr_send.at[c, n, source], gr_recv.at[c, n, source],
            "gr", lax.rem(g + n, gr),
        )

    def to_groups(c, source, src):
        for n in range(1, gr):
            gr_copy(c, n, source, src).start()

    def tp_start(c):
        for d in range(1, tp):

            @pl.when(t == f)
            def _():
                tp_copy(c, d, True).start()

            @pl.when(t != f)
            def _():
                tp_copy(c, d, False).start()

    def own_start(c):
        @pl.when(t != f)
        def _():
            fs_copy(c, 0, own(c, t), t).start()

        @pl.when(t == f)
        def _():
            pltpu.make_async_copy(own(c, t), bounce.at[c], load_sem.at[c]).start()
            to_groups(c, f, own(c, t))

    def own_store(c):
        @pl.when(t == f)
        def _():
            pltpu.make_async_copy(own(c, t), bounce.at[c], load_sem.at[c]).wait()
            pltpu.make_async_copy(bounce.at[c], out_rows(c, g, f), store_sem.at[c]).start()

    def tp_arrived(c):
        for d in range(1, tp):
            source = lax.rem(t + tp - d, tp)

            @pl.when(source == f)
            def _():
                tp_copy(c, d, True).wait_recv()
                to_groups(c, f, out_rows(c, g, f))

            @pl.when(source != f)
            def _():
                remote(
                    own(c, t), relay(c, source), tp_send.at[c, d], tp_recv.at[c, d], "tp", source
                ).wait_recv()
                fs_copy(c, d, relay(c, source), source).start()

    def fs_arrived(c):
        for d in range(1, fs):
            source = lax.rem(f + d, fs)
            remote(
                own(c, t), out_rows(c, g, source), fs_send.at[c, 0], fs_recv.at[c, source],
                "fs", source,
            ).wait_recv()
            to_groups(c, source, out_rows(c, g, source))

    def gr_arrived(c):
        for n in range(1, gr):
            for source in range(fs):
                group = lax.rem(g + gr - n, gr)
                remote(
                    own(c, t), out_rows(c, group, source), gr_send.at[c, n, source],
                    gr_recv.at[c, n, source], "gr", group,
                ).wait_recv()

    def own_stored(c):
        @pl.when(t == f)
        def _():
            pltpu.make_async_copy(bounce.at[c], out_rows(c, g, f), store_sem.at[c]).wait()

    def sent(c):
        for n in range(1, gr):
            for source in range(fs):
                gr_copy(c, n, source, out_rows(c, g, source)).wait_send()
        for d in range(1, tp):
            tp_copy(c, d, False).wait_send()
        for d in range(tp):
            target = lax.rem(t + tp - d, tp)

            @pl.when(target != f)
            def _():
                fs_copy(c, d, own(c, t), target).wait_send()

    def pick_slots(j):
        @pl.loop(0, tp)
        def _(b):
            base = (t * local_experts + j) * capacity
            index = lax.broadcasted_iota(jnp.int32, (capacity, token_rows), 0) + base
            first = place_of[b, 0:1, :] == index
            second = place_of[b, 1:2, :] == index
            share = jnp.where(first, share_of[b, 0:1, :], 0.0)
            share = share + jnp.where(second, share_of[b, 1:2, :], 0.0)
            share = jnp.sum(share, axis=1, keepdims=True)
            at = pl.ds(pl.multiple_of(b * capacity, capacity), capacity)
            slot_share[at, :] = jnp.broadcast_to(share, (capacity, 128))
            pick = jnp.where(first | second, 1.0, 0.0).astype(jnp.bfloat16)
            picks[b] = pick
            squares = jnp.zeros((capacity, 1), jnp.float32)
            for q in range(fs):
                columns = slice(q * features, (q + 1) * features)
                raw = jnp.dot(
                    pick, gathered[b, :, columns], preferred_element_type=jnp.float32
                )
                slots[at, columns] = raw.astype(jnp.bfloat16)
                squares = squares + jnp.sum(raw * raw, axis=1, keepdims=True)
            scale = lax.rsqrt(squares / width + norm_eps)
            for q in range(fs):
                columns = slice(q * features, (q + 1) * features)
                raw = slots[at, columns].astype(jnp.float32)
                slots[at, columns] = (raw * scale).astype(jnp.bfloat16)

    def weight_load(w, j):
        return pltpu.make_async_copy(outs[w].at[j], (gate_buf, up_buf)[w], weight_sem.at[w])

    def hidden_of(j):
        units = gate_buf.shape[0]
        step = 2 * capacity
        for start in range(0, units, 256):
            cut = slice(start, min(start + 256, units))

            @pl.loop(0, tp * capacity // step)
            def _(m):
                at = pl.ds(pl.multiple_of(m * step, step), step)
                into = (((1,), (1,)), ((), ()))
                gate = lax.dot_general(
                    slots[at, :], gate_buf[cut, :], into, preferred_element_type=jnp.float32
                )
                up = lax.dot_general(
                    slots[at, :], up_buf[cut, :], into, preferred_element_type=jnp.float32
                )
                value = gate / (1.0 + jnp.exp(-gate)) * up
                hid[at, cut] = (value * slot_share[at, 0:1]).astype(jnp.bfloat16)

    def hidden_to_tokens(j):
        @pl.loop(0, tp)
        def _(b):
            at = pl.ds(pl.multiple_of(b * capacity, capacity), capacity)
            spread_hid[j, b] = lax.dot_general(
                picks[b], hid[at, :], (((0,), (0,)), ((), ())),
                preferred_element_type=jnp.float32,
            ).astype(jnp.bfloat16)

    def down_load(r, j):
        start = pl.multiple_of(r * rows, rows)
        return pltpu.make_async_copy(
            outs[2].at[j, :, pl.ds(start, rows)], down_buf.at[r % 2, j], down_sem.at[r % 2, j]
        )

    def part_store(r, b):
        start = pl.multiple_of(r * rows, rows)
        return pltpu.make_async_copy(
            part_buf.at[r % 2, b], partial.at[b, :, pl.ds(start, rows)], part_sem.at[r % 2, b]
        )

    def part_of(r):
        @pl.loop(0, tp)
        def _(b):
            value = jnp.dot(
                spread_hid[0, b], down_buf[r % 2, 0], preferred_element_type=jnp.float32
            )
            for j in range(1, local_experts):
                value = value + jnp.dot(
                    spread_hid[j, b], down_buf[r % 2, j], preferred_element_type=jnp.float32
                )
            part_buf[r % 2, b] = value.astype(jnp.bfloat16)
            part_store(r, b).start()

    for d in range(1, fs):
        tokz(d).start()
    for copy in own_copies():
        copy.start()
    own_start(0)
    for d in range(1, tp):
        for k in range(2):
            info(d, k).start()
    tp_start(0)
    for copy in own_copies():
        copy.wait()
    for d in range(1, tp):
        tokt(d, f).start()
    ahead = min(3, total)
    for c in range(1, ahead):
        tp_start(c)
    for d in range(1, fs):
        source, copy = tokz_from(d)
        copy.wait_recv()
        for e in range(1, tp):
            tokt(e, source).start()

    for c in range(total + 1):
        if c + ahead < total:
            tp_start(c + ahead)
        if c + 1 < total:
            own_start(c + 1)
        if c < total:
            own_store(c)
            tp_arrived(c)
        if c >= 1:
            fs_arrived(c - 1)
    for c in range(total):
        gr_arrived(c)
        own_stored(c)

    for d in range(1, tp):
        source = lax.rem(t + d, tp)
        for k in range(2):
            whole = (place_of, share_of)[k]
            remote(
                (places, shares)[k], whole.at[source], info_send.at[d, k],
                info_recv.at[source, k], "tp", source,
            ).wait_recv()
        for s in range(fs):
            remote(
                slab(source, s), slab(source, s), tokt_send.at[d, s], tokt_recv.at[source, s],
                "tp", source,
            ).wait_recv()
    for j in range(local_experts):
        weight_load(0, j).start()
        weight_load(1, j).start()
        pick_slots(j)
        weight_load(0, j).wait()
        weight_load(1, j).wait()
        hidden_of(j)
        hidden_to_tokens(j)
    blocks_down = gr * fs
    for r in range(blocks_down):
        for j in range(local_experts):
            if r == 0:
                down_load(r, j).start()
            if r + 1 < blocks_down:
                down_load(r + 1, j).start()
        for j in range(local_experts):
            down_load(r, j).wait()
        if r >= 2:
            for b in range(tp):
                part_store(r - 2, b).wait()
        part_of(r)
    for r in range(max(0, blocks_down - 2), blocks_down):
        for b in range(tp):
            part_store(r, b).wait()

    for c in range(total):
        sent(c)
    for d in range(1, fs):
        tokz(d).wait_send()
    for d in range(1, tp):
        for s in range(fs):
            tokt(d, s).wait_send()
        for k in range(2):
            info(d, k).wait_send()


def serve(tokens, places, shares, capacity, *weights):
    gr, fs, tp = lax.axis_size("gr"), lax.axis_size("fs"), lax.axis_size("tp")
    experts, rows, columns = weights[0].shape
    local_experts = experts // tp
    token_rows, features = tokens.shape
    width = features * fs
    parts = [w.transpose(0, 2, 1) for w in weights]
    total = 3 * local_experts
    block = (columns, rows)
    bf16, f32 = jnp.bfloat16, jnp.float32
    served = jax.ShapeDtypeStruct((local_experts, columns, width), bf16)
    relayed = jax.ShapeDtypeStruct((local_experts, tp, *block), bf16)
    dma = pltpu.SemaphoreType.DMA
    anywhere = pl.BlockSpec(memory_space=pl.ANY)
    slots = tp * capacity
    found = pl.pallas_call(
        functools.partial(serve_kernel, (gr, fs, tp, local_experts, rows, capacity)),
        out_shape=[served] * 3
        + [relayed] * 3
        + [jax.ShapeDtypeStruct((tp, token_rows, width), bf16)],
        in_specs=[anywhere] * 6,
        out_specs=[anywhere] * 7,
        scratch_shapes=[
            pltpu.VMEM((total, *block), bf16),
            pltpu.VMEM((tp, token_rows, width), bf16),
            pltpu.VMEM((tp, *places.shape), jnp.int32),
            pltpu.VMEM((tp, *shares.shape), f32),
            pltpu.VMEM((tp, capacity, token_rows), bf16),
            pltpu.VMEM((slots, 128), f32),
            pltpu.VMEM((slots, width), bf16),
            pltpu.VMEM((slots, columns), bf16),
            pltpu.VMEM((local_experts, tp, token_rows, columns), bf16),
            pltpu.VMEM((columns, width), bf16),
            pltpu.VMEM((columns, width), bf16),
            pltpu.VMEM((2, local_experts, columns, rows), bf16),
            pltpu.VMEM((2, tp, token_rows, rows), bf16),
            dma((total, tp)),
            dma((total, tp)),
            dma((total, tp)),
            dma((total, fs)),
            dma((total, gr, fs)),
            dma((total, gr, fs)),
            dma((total,)),
            dma((total,)),
            dma((fs,)),
            dma((fs,)),
            dma((tp, fs)),
            dma((tp, fs)),
            dma((tp, 2)),
            dma((tp, 2)),
            dma((3,)),
            dma((2,)),
            dma((2, local_experts)),
            dma((2, tp)),
        ],
        compiler_params=pltpu.CompilerParams(
            collective_id=0, has_side_effects=True, vmem_limit_bytes=60 * 1024 * 1024
        ),
        name="serve",
    )(tokens, places, shares, *parts)
    return [w.swapaxes(1, 2) for w in found[:3]], found[6]


def combine_kernel(sizes, *refs):
    fs, tp = sizes
    partial, out = refs[:2]
    (
        mine, arrived, shared, reduced, total,
        load_sem, tp_send, tp_recv, fs_send, fs_recv, store_sem,
    ) = refs[2:]
    f, t = lax.axis_index("fs"), lax.axis_index("tp")
    features = out.shape[1]

    barrier = pltpu.get_barrier_semaphore()
    for axis, me, size in (("fs", f, fs), ("tp", t, tp)):
        for d in range(1, size):
            pl.semaphore_signal(
                barrier, inc=1, device_id={axis: lax.rem(me + d, size)}, device_id_type=MESH
            )
    pl.semaphore_wait(barrier, fs + tp - 2)

    def cut(block, q):
        start = pl.multiple_of(q * features, features)
        return partial.at[block, :, pl.ds(start, features)]

    def tp_copy(e, d):
        q = lax.rem(f + e, fs)
        target = lax.rem(t + d, tp)
        return pltpu.make_async_remote_copy(
            src_ref=cut(target, q), dst_ref=arrived.at[e % fs, d], send_sem=tp_send.at[e % fs, d],
            recv_sem=tp_recv.at[e % fs, d], device_id={"tp": target}, device_id_type=MESH,
        )

    def load(e):
        return pltpu.make_async_copy(
            cut(t, lax.rem(f + e, fs)), mine.at[e % fs], load_sem.at[e % fs]
        )

    def fs_copy(e):
        return pltpu.make_async_remote_copy(
            src_ref=shared.at[e], dst_ref=reduced.at[e], send_sem=fs_send.at[e],
            recv_sem=fs_recv.at[e], device_id={"fs": lax.rem(f + e, fs)}, device_id_type=MESH,
        )

    order = list(range(1, fs)) + [fs]
    for e in order:
        load(e).start()
        for d in range(1, tp):
            tp_copy(e, d).start()
    for e in order:
        load(e).wait()
        for d in range(1, tp):
            tp_copy(e, d).wait_recv()
        value = mine[e % fs].astype(jnp.float32)
        for d in range(1, tp):
            value = value + arrived[e % fs, d].astype(jnp.float32)
        if e < fs:
            shared[e] = value.astype(jnp.bfloat16)
            fs_copy(e).start()
        else:
            total[...] = value
    value = total[...]
    for e in range(1, fs):
        fs_copy(e).wait_recv()
        value = value + reduced[e].astype(jnp.float32)
    mine[0] = value.astype(jnp.bfloat16)
    store = pltpu.make_async_copy(mine.at[0], out, store_sem)
    store.start()
    for e in order:
        for d in range(1, tp):
            tp_copy(e, d).wait_send()
        if e < fs:
            fs_copy(e).wait_send()
    store.wait()


def combine(partial):
    fs, tp = lax.axis_size("fs"), lax.axis_size("tp")
    _, token_rows, width = partial.shape
    features = width // fs
    block = (token_rows, features)
    bf16 = jnp.bfloat16
    dma = pltpu.SemaphoreType.DMA
    return pl.pallas_call(
        functools.partial(combine_kernel, (fs, tp)),
        out_shape=jax.ShapeDtypeStruct(block, bf16),
        in_specs=[pl.BlockSpec(memory_space=pl.ANY)],
        out_specs=pl.BlockSpec(memory_space=pl.ANY),
        scratch_shapes=[
            pltpu.VMEM((fs, *block), bf16),
            pltpu.VMEM((fs, tp, *block), bf16),
            pltpu.VMEM((fs, *block), bf16),
            pltpu.VMEM((fs, *block), bf16),
            pltpu.VMEM(block, jnp.float32),
            dma((fs,)),
            dma((fs, tp)),
            dma((fs, tp)),
            dma((fs,)),
            dma((fs,)),
            dma,
        ],
        compiler_params=pltpu.CompilerParams(
            collective_id=1, has_side_effects=True, vmem_limit_bytes=48 * 1024 * 1024
        ),
        name="combine",
    )(partial)


def local(tokens, routes, route_weight, norm_gain, gate_master, up_master, down_master):
    experts, rows, columns = gate_master.shape
    gr, fs, tp = lax.axis_size("gr"), lax.axis_size("fs"), lax.axis_size("tp")
    token_rows, features = tokens.shape
    capacity = 3 * token_rows // experts
    fits = fs == tp and rows % 128 == 0 and features % 128 == 0 and features % rows == 0
    if not (fits and gr == 2 and capacity % 16 == 0 and columns % 16 == 0):
        return local_by_collectives(
            tokens, routes, route_weight, norm_gain, gate_master, up_master, down_master
        )
    scaled_gain = norm_gain[None, :, None]
    gate_w = (gate_master * scaled_gain).astype(jnp.bfloat16)
    up_w = (up_master * scaled_gain).astype(jnp.bfloat16)
    down_w = down_master.astype(jnp.bfloat16)
    places = slot_places(routes, experts, capacity)
    shares = jnp.pad(route_weight.T, ((0, 6), (0, 0)))
    served, partial = serve(tokens, places, shares, capacity, gate_w, up_w, down_w)
    return (combine(partial), *served)


def solution(mesh):
    placed = (
        P(("gr", "tp"), "fs"),
        P(("gr", "tp"), None),
        P(("gr", "tp"), None),
        P(("gr", "fs")),
        P(None, ("gr", "fs"), "tp"),
        P(None, ("gr", "fs"), "tp"),
        P(None, ("gr", "fs"), "tp"),
    )
    return jax.shard_map(
        local,
        mesh=mesh,
        in_specs=placed,
        out_specs=(
            P(("gr", "tp"), "fs"),
            P("tp", None, "fs"),
            P("tp", None, "fs"),
            P("tp", None, "fs"),
        ),
        check_vma=False,
    )
```

```python
import functools

import jax
import jax.numpy as jnp
from jax import lax
from jax.experimental import pallas as pl
from jax.experimental.pallas import tpu as pltpu
from jax.sharding import PartitionSpec as P

norm_eps = 1e-06
MESH = pl.DeviceIdType.MESH


def slot_table(routes, experts, capacity):
    flat_routes = routes.reshape(-1)
    onehot = (flat_routes[:, None] == jnp.arange(experts, dtype=jnp.int32)[None, :]).astype(
        jnp.int32
    )
    running = jnp.cumsum(onehot, axis=0)
    slot_index = jnp.sum(onehot * (running - 1), axis=1)
    return flat_routes * capacity + slot_index


def spread_kernel(sizes, count, flipped, *refs):
    gr, fs, tp, sub, local_experts, rows = sizes
    ins, outs, relays = refs[:count], refs[count : 2 * count], refs[2 * count : 3 * count]
    bounce, tp_send, tp_recv, fs_send, fs_recv, gr_send, gr_recv, load_sem, store_sem = refs[
        3 * count :
    ]
    g, f, t = lax.axis_index("gr"), lax.axis_index("fs"), lax.axis_index("tp")
    blocks = [(w, j) for j in range(local_experts) for w in range(count)]

    barrier = pltpu.get_barrier_semaphore()
    for axis, me, size in (("gr", g, gr), ("fs", f, fs), ("tp", t, tp)):
        for d in range(1, size):
            pl.semaphore_signal(
                barrier, inc=1, device_id={axis: lax.rem(me + d, size)}, device_id_type=MESH
            )
    pl.semaphore_wait(barrier, gr + fs + tp - 3)

    def out_rows(c, group, source):
        w, j = blocks[c]
        start = pl.multiple_of((group * fs + source) * rows, rows)
        if flipped:
            return outs[w].at[j, :, pl.ds(start, rows)]
        return outs[w].at[j, pl.ds(start, rows)]

    def own(c, target, s):
        w, j = blocks[c]
        return ins[w].at[s, target * local_experts + j]

    def relay(c, source, s):
        w, j = blocks[c]
        return relays[w].at[j, source, s]

    def tp_copy(c, d, s, to_out):
        target = lax.rem(t + d, tp)
        return pltpu.make_async_remote_copy(
            src_ref=own(c, target, s),
            dst_ref=out_rows(c, g, f) if to_out else relay(c, t, s),
            send_sem=tp_send.at[c, d, s],
            recv_sem=tp_recv.at[c, d, s],
            device_id={"tp": target},
            device_id_type=MESH,
        )

    def fs_copy(c, d, s, src, target):
        return pltpu.make_async_remote_copy(
            src_ref=src,
            dst_ref=out_rows(c, g, f),
            send_sem=fs_send.at[c, d, s],
            recv_sem=fs_recv.at[c, f],
            device_id={"fs": target},
            device_id_type=MESH,
        )

    def gr_copy(c, n, source, src):
        return pltpu.make_async_remote_copy(
            src_ref=src,
            dst_ref=out_rows(c, g, source),
            send_sem=gr_send.at[c, n, source],
            recv_sem=gr_recv.at[c, n, source],
            device_id={"gr": lax.rem(g + n, gr)},
            device_id_type=MESH,
        )

    def to_groups(c, source, src):
        for n in range(1, gr):
            gr_copy(c, n, source, src).start()

    def tp_start(c):
        for d in range(1, tp):
            for s in range(sub):

                @pl.when(t * sub + s == f)
                def _():
                    tp_copy(c, d, s, True).start()

                @pl.when(t * sub + s != f)
                def _():
                    tp_copy(c, d, s, False).start()

    def own_start(c):
        for s in range(sub):
            target = t * sub + s

            @pl.when(target != f)
            def _():
                fs_copy(c, 0, s, own(c, t, s), target).start()

            @pl.when(target == f)
            def _():
                pltpu.make_async_copy(own(c, t, s), bounce.at[c], load_sem.at[c]).start()
                to_groups(c, f, own(c, t, s))

    def own_store(c):
        for s in range(sub):

            @pl.when(t * sub + s == f)
            def _():
                pltpu.make_async_copy(own(c, t, s), bounce.at[c], load_sem.at[c]).wait()
                pltpu.make_async_copy(bounce.at[c], out_rows(c, g, f), store_sem.at[c]).start()

    def tp_arrived(c):
        for d in range(1, tp):
            source = lax.rem(t + tp - d, tp)
            for s in range(sub):
                target = source * sub + s

                @pl.when(target == f)
                def _():
                    tp_copy(c, d, s, True).wait_recv()
                    to_groups(c, f, out_rows(c, g, f))

                @pl.when(target != f)
                def _():
                    pltpu.make_async_remote_copy(
                        src_ref=own(c, t, s),
                        dst_ref=relay(c, source, s),
                        send_sem=tp_send.at[c, d, s],
                        recv_sem=tp_recv.at[c, d, s],
                        device_id={"tp": source},
                        device_id_type=MESH,
                    ).wait_recv()
                    fs_copy(c, d, s, relay(c, source, s), target).start()

    def fs_arrived(c):
        for d in range(1, fs):
            source = lax.rem(f + d, fs)
            pltpu.make_async_remote_copy(
                src_ref=own(c, t, 0),
                dst_ref=out_rows(c, g, source),
                send_sem=fs_send.at[c, 0, 0],
                recv_sem=fs_recv.at[c, source],
                device_id={"fs": source},
                device_id_type=MESH,
            ).wait_recv()
            to_groups(c, source, out_rows(c, g, source))

    total = len(blocks)
    ahead = min(3, total)
    own_start(0)
    for c in range(ahead):
        tp_start(c)
    for c in range(total + 1):
        if c + ahead < total:
            tp_start(c + ahead)
        if c + 1 < total:
            own_start(c + 1)
        if c < total:
            own_store(c)
            tp_arrived(c)
        if c >= 1:
            fs_arrived(c - 1)

    for c in range(total):
        for n in range(1, gr):
            for source in range(fs):
                group = lax.rem(g + gr - n, gr)
                pltpu.make_async_remote_copy(
                    src_ref=own(c, t, 0),
                    dst_ref=out_rows(c, group, source),
                    send_sem=gr_send.at[c, n, source],
                    recv_sem=gr_recv.at[c, n, source],
                    device_id={"gr": group},
                    device_id_type=MESH,
                ).wait_recv()
                gr_copy(c, n, source, out_rows(c, g, source)).wait_send()
        for s in range(sub):
            for d in range(1, tp):
                tp_copy(c, d, s, False).wait_send()
            for d in range(tp):
                target = lax.rem(t + tp - d, tp) * sub + s

                @pl.when(target != f)
                def _():
                    fs_copy(c, d, s, own(c, t, s), target).wait_send()

            @pl.when(t * sub + s == f)
            def _():
                pltpu.make_async_copy(bounce.at[c], out_rows(c, g, f), store_sem.at[c]).wait()


def spread(*weights):
    gr, fs, tp = lax.axis_size("gr"), lax.axis_size("fs"), lax.axis_size("tp")
    experts, rows, columns = weights[0].shape
    local_experts = experts // tp
    assert fs % tp == 0
    sub = fs // tp
    width = columns // sub
    count = len(weights)
    total = count * local_experts
    flipped = rows % 128 == 0
    order = (2, 0, 3, 1) if flipped else (2, 0, 1, 3)
    parts = [w.reshape(experts, rows, sub, width).transpose(order) for w in weights]
    block = (width, rows) if flipped else (rows, width)
    whole = (width, gr * fs * rows) if flipped else (gr * fs * rows, width)
    served = jax.ShapeDtypeStruct((local_experts, *whole), jnp.bfloat16)
    relayed = jax.ShapeDtypeStruct((local_experts, tp, sub, *block), jnp.bfloat16)
    dma = pltpu.SemaphoreType.DMA
    sent = 2 * total * rows * columns * (tp - 1 + fs - 1 + (gr - 1) * fs) // fs
    found = pl.pallas_call(
        functools.partial(spread_kernel, (gr, fs, tp, sub, local_experts, rows), count, flipped),
        out_shape=[served] * count + [relayed] * count,
        in_specs=[pl.BlockSpec(memory_space=pl.ANY)] * count,
        out_specs=[pl.BlockSpec(memory_space=pl.ANY)] * (2 * count),
        scratch_shapes=[
            pltpu.VMEM((total, *block), jnp.bfloat16),
            dma((total, tp, sub)),
            dma((total, tp, sub)),
            dma((total, tp, sub)),
            dma((total, fs)),
            dma((total, gr, fs)),
            dma((total, gr, fs)),
            dma((total,)),
            dma((total,)),
        ],
        compiler_params=pltpu.CompilerParams(collective_id=0, has_side_effects=True),
        cost_estimate=pl.CostEstimate(flops=0, bytes_accessed=40 * sent, transcendentals=0),
    )(*parts)
    return [w.swapaxes(1, 2) if flipped else w for w in found[:count]]


def local_by_collectives(tokens, routes, route_weight, norm_gain, gate_master, up_master, down_master):
    experts = gate_master.shape[0]
    tp_count = lax.axis_size("tp")
    fs_count = lax.axis_size("fs")
    local_experts = experts // tp_count
    token_rows = tokens.shape[0]
    model_width = tokens.shape[1] * fs_count
    capacity = 3 * token_rows // experts
    scaled_gain = norm_gain[None, :, None]
    gate_w = (gate_master * scaled_gain).astype(jnp.bfloat16)
    up_w = (up_master * scaled_gain).astype(jnp.bfloat16)
    down_w = down_master.astype(jnp.bfloat16)
    gate_w, up_w, down_w = spread(gate_w, up_w, down_w)
    as_float = tokens.astype(jnp.float32)
    square_total = lax.psum(jnp.sum(as_float * as_float, axis=1), "fs")
    normed = (as_float * lax.rsqrt(square_total / model_width + norm_eps)[:, None]).astype(
        jnp.bfloat16
    )
    placing = slot_table(routes, experts, capacity)
    slot_rows = jnp.arange(experts * capacity, dtype=jnp.int32)
    picked = (slot_rows[:, None] == placing[None, :]).reshape(experts * capacity, token_rows, 2)
    route_table = jnp.sum(picked.astype(jnp.float32), axis=2).astype(jnp.bfloat16)
    outgoing = jnp.dot(route_table, normed, preferred_element_type=jnp.float32).astype(jnp.bfloat16)
    outgoing = outgoing.reshape(tp_count, local_experts, capacity, tokens.shape[1])
    shard_piece = lax.all_gather(
        lax.all_to_all(outgoing, "tp", split_axis=0, concat_axis=0, tiled=True),
        "fs",
        axis=3,
        tiled=True,
    )
    returned = []
    for j in range(local_experts):
        rows = shard_piece[:, j]
        gate_acc = jnp.einsum("scd,df->scf", rows, gate_w[j], preferred_element_type=jnp.float32)
        up_acc = jnp.einsum("scd,df->scf", rows, up_w[j], preferred_element_type=jnp.float32)
        hidden = (jax.nn.silu(gate_acc) * up_acc).astype(jnp.bfloat16)
        partial_value = jnp.einsum(
            "scf,df->scd", hidden, down_w[j], preferred_element_type=jnp.float32
        )
        summed = lax.psum_scatter(
            partial_value.astype(jnp.bfloat16), "fs", scatter_dimension=2, tiled=True
        )
        returned.append(lax.all_to_all(summed, "tp", split_axis=0, concat_axis=0, tiled=True))
    produced = jnp.stack(returned, axis=1)
    produced = produced.reshape(experts * capacity, produced.shape[3])
    pair_slots = placing.reshape(token_rows, 2)
    first_rows = jnp.take(produced, pair_slots[:, 0], axis=0)
    second_rows = jnp.take(produced, pair_slots[:, 1], axis=0)
    mixed_out = first_rows * route_weight[:, 0:1] + second_rows * route_weight[:, 1:2]
    return (mixed_out.astype(jnp.bfloat16), gate_w, up_w, down_w)


def slot_places(routes, experts, capacity):
    rows = routes.shape[0]
    hits = (routes[:, :, None] == jnp.arange(experts, dtype=jnp.int32)).astype(jnp.int32)
    both = hits[:, 0] + hits[:, 1]
    before = jnp.cumsum(both, axis=0) - both
    first = jnp.sum(hits[:, 0] * before, axis=1)
    second = jnp.sum(hits[:, 1] * (before + hits[:, 0]), axis=1)
    places = jnp.stack([first, second]) + routes.T * capacity
    return jnp.pad(places, ((0, 6), (0, 0)))


def serve_kernel(sizes, *refs):
    gr, fs, tp, local_experts, rows, capacity = sizes
    tokens, places, shares = refs[:3]
    ins, outs, relays, mixed = refs[3:6], refs[6:9], refs[9:12], refs[12]
    (
        bounce_in, bounce_down, gathered, place_of, share_of, picks, slot_share, slots, hid, spread_hid,
        gate_buf, up_buf, down_buf, part, from_core, to_side, from_side, to_fs, from_near,
        from_far, kept, kept_far, mixed_buf,
        tp_send, tp_recv, fs_send, fs_recv, gr_send, gr_recv, load_sem, store_sem,
        up_sem, low_sem, slab_recv, core_send, side_send, block_recv, info_send, info_recv,
        own_sem, weight_sem, down_sem, core_psend, core_precv, side_psend, side_precv,
        near_send, near_recv, far_send, far_recv, mixed_sem,
    ) = refs[13:]
    g, f, t = lax.axis_index("gr"), lax.axis_index("fs"), lax.axis_index("tp")
    bounce = (bounce_in, bounce_down)
    halves = 2
    half = rows // halves
    blocks = [(w, j) for j in range(local_experts) for w in range(2)]
    blocks += [(2, h) for h in range(halves)]
    total = len(blocks)
    token_rows, features = tokens.shape
    width = fs * features

    barrier = pltpu.get_barrier_semaphore()
    for axis, me, size in (("gr", g, gr), ("fs", f, fs), ("tp", t, tp)):
        for d in range(1, size):
            pl.semaphore_signal(
                barrier, inc=1, device_id={axis: lax.rem(me + d, size)}, device_id_type=MESH
            )
    pl.semaphore_wait(barrier, gr + fs + tp - 3)

    def remote(src, dst, send, recv, axis, target):
        return pltpu.make_async_remote_copy(
            src_ref=src, dst_ref=dst, send_sem=send, recv_sem=recv,
            device_id={axis: target}, device_id_type=MESH,
        )

    def slab(block, source):
        return gathered.at[block, source]

    core = t + 1 - 2 * lax.rem(t, 2)
    side = lax.rem(t + 2, tp)
    core_side = lax.rem(core + 2, tp)

    def slab_copy(source, up):
        mine = slab(t, source)
        sem = (up_sem if up else low_sem).at[source]
        return remote(mine, mine, sem, slab_recv.at[source], "fs", f + 1 if up else f - 1)

    def slab_pass(source, up):
        @pl.when(f < fs - 1 if up else f > 0)
        def _():
            slab_copy(source, up).start()

    def to_core(k, source):
        mine = slab((t, side)[k], source)
        return remote(
            mine, mine, core_send.at[k, source], block_recv.at[(t, side)[k], source], "tp", core
        )

    def to_sides(source):
        mine = slab(t, source)
        return remote(
            mine, mine, side_send.at[source], block_recv.at[t, source], "tp", side
        )

    def slab_spread(source):
        to_sides(source).start()
        to_core(0, source).start()

    def slab_arrived(k):
        for up in (True, False):
            source = f - k if up else f + k

            @pl.when(source >= 0 if up else source < fs)
            def _():
                slab_copy(source, up).wait_recv()
                slab_pass(source, up)
                slab_spread(source)

    def block_wait(block, source):
        mine = slab(block, source)
        remote(
            mine, mine, side_send.at[source], block_recv.at[block, source], "tp", side
        ).wait_recv()

    def side_arrived(k):
        source = lax.rem(f + k, fs)
        block_wait(side, source)
        to_core(1, source).start()

    def core_arrived():
        for block in (core, core_side):
            for source in range(fs):
                block_wait(block, source)
        for d in range(1, tp):
            source = lax.rem(t + d, tp)
            for k in range(2):
                whole = (place_of, share_of)[k]
                remote(
                    (places, shares)[k], whole.at[source], info_send.at[d, k],
                    info_recv.at[source, k], "tp", source,
                ).wait_recv()

    def info(d, k):
        whole = (place_of, share_of)[k]
        return remote(
            (places, shares)[k], whole.at[t], info_send.at[d, k], info_recv.at[t, k],
            "tp", lax.rem(t + d, tp),
        )

    def own_copies():
        return (
            pltpu.make_async_copy(tokens, slab(t, f), own_sem.at[0]),
            pltpu.make_async_copy(places, place_of.at[t], own_sem.at[1]),
            pltpu.make_async_copy(shares, share_of.at[t], own_sem.at[2]),
        )

    def out_rows(c, group, source):
        w, j = blocks[c]
        start = pl.multiple_of((group * fs + source) * rows, rows)
        if w == 2:
            return outs[w].at[:, :, pl.ds(start + j * half, half)]
        return outs[w].at[j, :, pl.ds(start, rows)]

    def own(c, target):
        w, j = blocks[c]
        if w == 2:
            first = target * local_experts
            return ins[w].at[pl.ds(first, local_experts), :, j * half : (j + 1) * half]
        return ins[w].at[target * local_experts + j]

    def relay(c, source):
        w, j = blocks[c]
        if w == 2:
            return relays[w].at[source, :, :, j * half : (j + 1) * half]
        return relays[w].at[j, source]

    def tp_copy(c, d, to_out):
        target = lax.rem(t + d, tp)
        return remote(
            own(c, target), out_rows(c, g, f) if to_out else relay(c, t),
            tp_send.at[c, d], tp_recv.at[c, d], "tp", target,
        )

    def fs_copy(c, d, src, target):
        return remote(src, out_rows(c, g, f), fs_send.at[c, d], fs_recv.at[c, f], "fs", target)

    def gr_copy(c, n, source, src):
        return remote(
            src, out_rows(c, g, source), gr_send.at[c, n, source], gr_recv.at[c, n, source],
            "gr", lax.rem(g + n, gr),
        )

    def to_groups(c, source, src):
        for n in range(1, gr):
            gr_copy(c, n, source, src).start()

    def tp_start(c):
        for d in range(1, tp):

            @pl.when(t == f)
            def _():
                tp_copy(c, d, True).start()

            @pl.when(t != f)
            def _():
                tp_copy(c, d, False).start()

    def bounce_of(c):
        w, j = blocks[c]
        return bounce[1].at[j] if w == 2 else bounce[0].at[c]

    def own_store(c):
        @pl.when(t == f)
        def _():
            pltpu.make_async_copy(own(c, t), bounce_of(c), load_sem.at[c]).wait()
            pltpu.make_async_copy(bounce_of(c), out_rows(c, g, f), store_sem.at[c]).start()

    def fs_send_next(c, k):
        odd = lax.rem(f, 2)
        source = lax.rem(f + (2, 3 - 2 * odd, 1 + 2 * odd)[k], fs)
        d = lax.rem(t - source + tp, tp)

        @pl.when(source == t)
        def _():
            fs_copy(c, d, own(c, t), source).start()

        @pl.when(source != t)
        def _():
            remote(
                own(c, t), relay(c, source), tp_send.at[c, d], tp_recv.at[c, d], "tp", source
            ).wait_recv()
            fs_copy(c, d, relay(c, source), source).start()

    def home(c):
        d = lax.rem(t - f + tp, tp)

        @pl.when(t == f)
        def _():
            pltpu.make_async_copy(own(c, t), bounce_of(c), load_sem.at[c]).start()
            to_groups(c, f, own(c, t))

        @pl.when(t != f)
        def _():
            tp_copy(c, d, True).wait_recv()
            to_groups(c, f, out_rows(c, g, f))

    def fs_arrived(c, k):
        odd = lax.rem(f, 2)
        source = lax.rem(f + (2, 3 - 2 * odd, 1 + 2 * odd)[k], fs)
        remote(
            own(c, t), out_rows(c, g, source), fs_send.at[c, 0], fs_recv.at[c, source],
            "fs", source,
        ).wait_recv()
        to_groups(c, source, out_rows(c, g, source))

    def gr_arrived(c):
        for n in range(1, gr):
            for source in range(fs):
                group = lax.rem(g + gr - n, gr)
                remote(
                    own(c, t), out_rows(c, group, source), gr_send.at[c, n, source],
                    gr_recv.at[c, n, source], "gr", group,
                ).wait_recv()

    def own_stored(c):
        @pl.when(t == f)
        def _():
            pltpu.make_async_copy(bounce_of(c), out_rows(c, g, f), store_sem.at[c]).wait()

    def sent(c):
        for n in range(1, gr):
            for source in range(fs):
                gr_copy(c, n, source, out_rows(c, g, source)).wait_send()
        for d in range(1, tp):
            tp_copy(c, d, False).wait_send()
        for d in range(tp):
            target = lax.rem(t + tp - d, tp)

            @pl.when(target != f)
            def _():
                fs_copy(c, d, own(c, t), target).wait_send()

    def pick_slots(j):
        @pl.loop(0, tp)
        def _(b):
            base = (t * local_experts + j) * capacity
            index = lax.broadcasted_iota(jnp.int32, (capacity, token_rows), 0) + base
            first = place_of[b, 0:1, :] == index
            second = place_of[b, 1:2, :] == index
            share = jnp.where(first, share_of[b, 0:1, :], 0.0)
            share = share + jnp.where(second, share_of[b, 1:2, :], 0.0)
            share = jnp.sum(share, axis=1, keepdims=True)
            at = pl.ds(pl.multiple_of(b * capacity, capacity), capacity)
            slot_share[at, :] = jnp.broadcast_to(share, (capacity, 128))
            pick = jnp.where(first | second, 1.0, 0.0).astype(jnp.bfloat16)
            picks[b] = pick
            squares = jnp.zeros((capacity, 1), jnp.float32)
            for q in range(fs):
                columns = slice(q * features, (q + 1) * features)
                raw = jnp.dot(
                    pick, gathered[b, q], preferred_element_type=jnp.float32
                )
                slots[at, columns] = raw.astype(jnp.bfloat16)
                squares = squares + jnp.sum(raw * raw, axis=1, keepdims=True)
            scale = lax.rsqrt(squares / width + norm_eps)
            for q in range(fs):
                columns = slice(q * features, (q + 1) * features)
                raw = slots[at, columns].astype(jnp.float32)
                slots[at, columns] = (raw * scale).astype(jnp.bfloat16)

    def weight_load(w, j):
        return pltpu.make_async_copy(outs[w].at[j], (gate_buf, up_buf)[w], weight_sem.at[w])

    def hidden_of(j, start):
        units = gate_buf.shape[0]
        step = 2 * capacity
        cut = slice(start, min(start + 256, units))

        @pl.loop(0, tp * capacity // step)
        def _(m):
            at = pl.ds(pl.multiple_of(m * step, step), step)
            into = (((1,), (1,)), ((), ()))
            gate = lax.dot_general(
                slots[at, :], gate_buf[cut, :], into, preferred_element_type=jnp.float32
            )
            up = lax.dot_general(
                slots[at, :], up_buf[cut, :], into, preferred_element_type=jnp.float32
            )
            value = gate / (1.0 + jnp.exp(-gate)) * up
            hid[at, cut] = (value * slot_share[at, 0:1]).astype(jnp.bfloat16)

    def hidden_to_tokens(j):
        @pl.loop(0, tp)
        def _(b):
            at = pl.ds(pl.multiple_of(b * capacity, capacity), capacity)
            spread_hid[j, b] = lax.dot_general(
                picks[b], hid[at, :], (((0,), (0,)), ((), ())),
                preferred_element_type=jnp.float32,
            ).astype(jnp.bfloat16)

    pieces = [(h, n) for h in range(halves) for n in range(fs)]
    upper = f // 2
    near = f + 1 - 2 * lax.rem(f, 2)
    inner = (f == 1) | (f == 2)

    def column_owner(n):
        return (3 - 3 * upper, 2 - upper, near, f)[n]

    joined = features // rows
    cut = joined * half

    def down_loads(p):
        h, n = pieces[p]
        q = column_owner(n)
        copies = []
        for i in range(joined):
            start = pl.multiple_of((q * joined + i) * rows, rows)
            copies.append(
                pltpu.make_async_copy(
                    outs[2].at[:, :, pl.ds(start + h * half, half)],
                    down_buf.at[p % 2, :, :, i * half : (i + 1) * half],
                    down_sem.at[p % 2, i],
                )
            )
        return copies

    def core_part(p, k):
        block = (core, core_side)[k]
        return remote(
            part.at[p, block], from_core.at[p, k], core_psend.at[p, k], core_precv.at[p, k],
            "tp", core,
        )

    def side_part(p):
        return remote(
            to_side.at[p], from_side.at[p], side_psend.at[p], side_precv.at[p], "tp", side
        )

    def near_part(p):
        return remote(to_fs.at[p], from_near.at[p], near_send.at[p], near_recv.at[p], "fs", near)

    def far_part(p):
        h, n = pieces[p]
        return remote(
            to_fs.at[p], from_far.at[h], far_send.at[p], far_recv.at[h], "fs", column_owner(n)
        )

    def piece_start(p):
        for copy in down_loads(p):
            copy.wait()
        if p + 1 < len(pieces) and pieces[p + 1][0] == pieces[p][0]:
            for copy in down_loads(p + 1):
                copy.start()

        @pl.loop(0, tp)
        def _(b):
            value = jnp.dot(
                spread_hid[0, b], down_buf[p % 2, 0], preferred_element_type=jnp.float32
            )
            for j in range(1, local_experts):
                value = value + jnp.dot(
                    spread_hid[j, b], down_buf[p % 2, j], preferred_element_type=jnp.float32
                )
            part[p, b] = value.astype(jnp.bfloat16)

        for k in range(2):
            core_part(p, k).start()

    def piece_side(p):
        for k in range(2):
            core_part(p, k).wait_recv()
        value = part[p, side].astype(jnp.float32) + from_core[p, 1].astype(jnp.float32)
        to_side[p] = value.astype(jnp.bfloat16)
        side_part(p).start()

    def piece_fs(p):
        h, n = pieces[p]
        side_part(p).wait_recv()
        value = part[p, t].astype(jnp.float32) + from_core[p, 0].astype(jnp.float32)
        value = value + from_side[p].astype(jnp.float32)
        if n == 3:
            kept[h] = value
        elif n == 2:
            to_fs[p] = value.astype(jnp.bfloat16)
            near_part(p).start()
        else:
            @pl.when(inner)
            def _():
                kept_far[p % 2] = value

            @pl.when(jnp.logical_not(inner))
            def _():
                to_fs[p] = value.astype(jnp.bfloat16)
                near_part(p).start()

    def piece_far(p):
        h, n = pieces[p]

        @pl.when(inner)
        def _():
            near_part(p).wait_recv()
            value = kept_far[p % 2] + from_near[p].astype(jnp.float32)
            to_fs[p] = value.astype(jnp.bfloat16)
            far_part(p).start()

    def finish(h):
        value = kept[h]
        near_part(h * fs + 2).wait_recv()
        value = value + from_near[h * fs + 2].astype(jnp.float32)
        far_part(h * fs).wait_recv()
        value = value + from_far[h].astype(jnp.float32)
        value = value.astype(jnp.bfloat16)
        for i in range(joined):
            first = i * rows + h * half
            mixed_buf[:, first : first + half] = value[:, i * half : (i + 1) * half]

    def all_pieces(h):
        own_pieces = [p for p in range(len(pieces)) if pieces[p][0] == h]
        thunks = [lambda: [copy.start() for copy in down_loads(own_pieces[0])]]
        for n in range(len(own_pieces) + 2):
            if n < len(own_pieces):
                thunks.append(functools.partial(piece_start, own_pieces[n]))
            if 1 <= n <= len(own_pieces):
                thunks.append(functools.partial(piece_side, own_pieces[n - 1]))
            if n >= 2:
                thunks.append(functools.partial(piece_fs, own_pieces[n - 2]))
            if n in (3, 4):
                thunks.append(functools.partial(piece_far, own_pieces[n - 3]))
        return thunks

    def expert_thunks(j):
        def begin():
            for w in range(2):
                gr_arrived(2 * j + w)
                own_stored(2 * j + w)
                weight_load(w, j).start()
            pick_slots(j)
            weight_load(0, j).wait()
            weight_load(1, j).wait()

        units = gate_buf.shape[0]
        cuts = [functools.partial(hidden_of, j, start) for start in range(0, units, 256)]
        return [begin, *cuts, functools.partial(hidden_to_tokens, j)]

    own_load = own_copies()
    for copy in own_load:
        copy.start()
    for up in (True, False):
        @pl.when(f < fs - 1 if up else f > 0)
        def _():
            remote(
                tokens, slab(t, f), (up_sem if up else low_sem).at[f], slab_recv.at[f],
                "fs", f + 1 if up else f - 1,
            ).start()
    for d in range(1, tp):
        for k in range(2):
            info(d, k).start()
    early = min(4, total)
    for c in range(early):
        tp_start(c)
    own_load[0].wait()
    slab_spread(f)

    def out_waits(c):
        return [
            functools.partial(home, c),
            *[functools.partial(fs_send_next, c, k) for k in range(fs - 1)],
        ]

    def fs_waits(c):
        return [functools.partial(fs_arrived, c, k) for k in range(fs - 1)]

    def mix(waits, todo):
        for n, wait in enumerate(waits):
            wait()
            take = -(-len(todo) // (len(waits) - n))
            for thunk in todo[:take]:
                thunk()
            todo = todo[take:]
        for thunk in todo:
            thunk()

    def both(first, second):
        longer = max(len(first), len(second))
        found = []
        for n in range(longer):
            found += first[n : n + 1] + second[n : n + 1]
        return found

    mix(out_waits(0), [])
    slab_arrived(1)
    mix(out_waits(1), [])
    slab_arrived(2)
    own_store(0)
    mix(both(fs_waits(0), out_waits(2)), [])
    slab_arrived(3)
    for c in range(early, total):
        tp_start(c)
    own_store(1)
    own_store(2)
    mix(both(fs_waits(1), out_waits(3)), [])
    own_load[1].wait()
    own_load[2].wait()
    for k in range(fs):
        side_arrived(k)
    own_store(3)
    mix(both(fs_waits(2), out_waits(4)), [])
    own_store(4)
    core_arrived()
    mix(both(fs_waits(3), out_waits(5)), expert_thunks(0))
    own_store(5)
    mix(fs_waits(4), expert_thunks(1))
    gr_arrived(4)
    own_stored(4)
    mix(fs_waits(5), all_pieces(0))
    for h in range(1, halves):
        c = 2 * local_experts + h
        gr_arrived(c)
        own_stored(c)
        for thunk in all_pieces(h):
            thunk()
    for h in range(halves):
        finish(h)
    store = pltpu.make_async_copy(mixed_buf, mixed, mixed_sem)
    store.start()

    for c in range(total):
        sent(c)
    for source in range(fs):
        for up in (True, False):
            @pl.when((f < fs - 1) & (source <= f) if up else (f > 0) & (source >= f))
            def _():
                slab_copy(source, up).wait_send()
        to_sides(source).wait_send()
        to_core(0, source).wait_send()
        to_core(1, source).wait_send()
    for d in range(1, tp):
        for k in range(2):
            info(d, k).wait_send()
    for p in range(len(pieces)):
        for k in range(2):
            core_part(p, k).wait_send()
        side_part(p).wait_send()
        if pieces[p][1] == 2:
            near_part(p).wait_send()
        elif pieces[p][1] < 2:
            @pl.when(inner)
            def _():
                far_part(p).wait_send()

            @pl.when(jnp.logical_not(inner))
            def _():
                near_part(p).wait_send()
    store.wait()


def serve(tokens, places, shares, capacity, *weights):
    gr, fs, tp = lax.axis_size("gr"), lax.axis_size("fs"), lax.axis_size("tp")
    experts, rows, columns = weights[0].shape
    local_experts = experts // tp
    token_rows, features = tokens.shape
    width = features * fs
    parts = [w.transpose(0, 2, 1) for w in weights]
    block = (columns, rows)
    bf16, f32 = jnp.bfloat16, jnp.float32
    served = jax.ShapeDtypeStruct((local_experts, columns, width), bf16)
    relayed = jax.ShapeDtypeStruct((local_experts, tp, *block), bf16)
    relayed_down = jax.ShapeDtypeStruct((tp, local_experts, *block), bf16)
    half, pieces = rows // 2, 2 * fs
    cut = features // rows * half
    total = 2 * local_experts + 2
    dma = pltpu.SemaphoreType.DMA
    anywhere = pl.BlockSpec(memory_space=pl.ANY)
    slots = tp * capacity
    found = pl.pallas_call(
        functools.partial(serve_kernel, (gr, fs, tp, local_experts, rows, capacity)),
        out_shape=[served] * 3
        + [relayed] * 2
        + [relayed_down, jax.ShapeDtypeStruct((token_rows, features), bf16)],
        in_specs=[anywhere] * 6,
        out_specs=[anywhere] * 7,
        scratch_shapes=[
            pltpu.VMEM((2 * local_experts, *block), bf16),
            pltpu.VMEM((2, local_experts, columns, half), bf16),
            pltpu.VMEM((tp, fs, token_rows, features), bf16),
            pltpu.VMEM((tp, *places.shape), jnp.int32),
            pltpu.VMEM((tp, *shares.shape), f32),
            pltpu.VMEM((tp, capacity, token_rows), bf16),
            pltpu.VMEM((slots, 128), f32),
            pltpu.VMEM((slots, width), bf16),
            pltpu.VMEM((slots, columns), bf16),
            pltpu.VMEM((local_experts, tp, token_rows, columns), bf16),
            pltpu.VMEM((columns, width), bf16),
            pltpu.VMEM((columns, width), bf16),
            pltpu.VMEM((2, local_experts, columns, cut), bf16),
            pltpu.VMEM((pieces, tp, token_rows, cut), bf16),
            pltpu.VMEM((pieces, 2, token_rows, cut), bf16),
            pltpu.VMEM((pieces, token_rows, cut), bf16),
            pltpu.VMEM((pieces, token_rows, cut), bf16),
            pltpu.VMEM((pieces, token_rows, cut), bf16),
            pltpu.VMEM((pieces, token_rows, cut), bf16),
            pltpu.VMEM((2, token_rows, cut), bf16),
            pltpu.VMEM((2, token_rows, cut), f32),
            pltpu.VMEM((2, token_rows, cut), f32),
            pltpu.VMEM((token_rows, features), bf16),
            dma((total, tp)),
            dma((total, tp)),
            dma((total, tp)),
            dma((total, fs)),
            dma((total, gr, fs)),
            dma((total, gr, fs)),
            dma((total,)),
            dma((total,)),
            dma((fs,)),
            dma((fs,)),
            dma((fs,)),
            dma((2, fs)),
            dma((fs,)),
            dma((tp, fs)),
            dma((tp, 2)),
            dma((tp, 2)),
            dma((3,)),
            dma((2,)),
            dma((2, features // rows)),
            dma((pieces, 2)),
            dma((pieces, 2)),
            dma((pieces,)),
            dma((pieces,)),
            dma((pieces,)),
            dma((pieces,)),
            dma((pieces,)),
            dma((2,)),
            dma,
        ],
        compiler_params=pltpu.CompilerParams(
            collective_id=0, has_side_effects=True, vmem_limit_bytes=60 * 1024 * 1024
        ),
        name="serve",
    )(tokens, places, shares, *parts)
    return [w.swapaxes(1, 2) for w in found[:3]], found[6]


def local(tokens, routes, route_weight, norm_gain, gate_master, up_master, down_master):
    experts, rows, columns = gate_master.shape
    gr, fs, tp = lax.axis_size("gr"), lax.axis_size("fs"), lax.axis_size("tp")
    token_rows, features = tokens.shape
    capacity = 3 * token_rows // experts
    fits = fs == tp and rows % 128 == 0 and features % 128 == 0 and features % rows == 0
    if not (fits and tp == 4 and rows % 256 == 0 and capacity % 16 == 0 and columns % 16 == 0):
        return local_by_collectives(
            tokens, routes, route_weight, norm_gain, gate_master, up_master, down_master
        )
    scaled_gain = norm_gain[None, :, None]
    gate_w = (gate_master * scaled_gain).astype(jnp.bfloat16)
    up_w = (up_master * scaled_gain).astype(jnp.bfloat16)
    down_w = down_master.astype(jnp.bfloat16)
    places = slot_places(routes, experts, capacity)
    shares = jnp.pad(route_weight.T, ((0, 6), (0, 0)))
    served, mixed = serve(tokens, places, shares, capacity, gate_w, up_w, down_w)
    return (mixed, *served)


def solution(mesh):
    placed = (
        P(("gr", "tp"), "fs"),
        P(("gr", "tp"), None),
        P(("gr", "tp"), None),
        P(("gr", "fs")),
        P(None, ("gr", "fs"), "tp"),
        P(None, ("gr", "fs"), "tp"),
        P(None, ("gr", "fs"), "tp"),
    )
    return jax.shard_map(
        local,
        mesh=mesh,
        in_specs=placed,
        out_specs=(
            P(("gr", "tp"), "fs"),
            P("tp", None, "fs"),
            P("tp", None, "fs"),
            P("tp", None, "fs"),
        ),
        check_vma=False,
    )
```

```python
import functools

import jax
import jax.numpy as jnp
from jax import lax
from jax.experimental import pallas as pl
from jax.experimental.pallas import tpu as pltpu
from jax.sharding import PartitionSpec as P

norm_eps = 1e-06
MESH = pl.DeviceIdType.MESH


def slot_table(routes, experts, capacity):
    flat_routes = routes.reshape(-1)
    onehot = (flat_routes[:, None] == jnp.arange(experts, dtype=jnp.int32)[None, :]).astype(
        jnp.int32
    )
    running = jnp.cumsum(onehot, axis=0)
    slot_index = jnp.sum(onehot * (running - 1), axis=1)
    return flat_routes * capacity + slot_index


def spread_kernel(sizes, count, flipped, *refs):
    gr, fs, tp, sub, local_experts, rows = sizes
    ins, outs, relays = refs[:count], refs[count : 2 * count], refs[2 * count : 3 * count]
    bounce, tp_send, tp_recv, fs_send, fs_recv, gr_send, gr_recv, load_sem, store_sem = refs[
        3 * count :
    ]
    g, f, t = lax.axis_index("gr"), lax.axis_index("fs"), lax.axis_index("tp")
    blocks = [(w, j) for j in range(local_experts) for w in range(count)]

    barrier = pltpu.get_barrier_semaphore()
    for axis, me, size in (("gr", g, gr), ("fs", f, fs), ("tp", t, tp)):
        for d in range(1, size):
            pl.semaphore_signal(
                barrier, inc=1, device_id={axis: lax.rem(me + d, size)}, device_id_type=MESH
            )
    pl.semaphore_wait(barrier, gr + fs + tp - 3)

    def out_rows(c, group, source):
        w, j = blocks[c]
        start = pl.multiple_of((group * fs + source) * rows, rows)
        if flipped:
            return outs[w].at[j, :, pl.ds(start, rows)]
        return outs[w].at[j, pl.ds(start, rows)]

    def own(c, target, s):
        w, j = blocks[c]
        return ins[w].at[s, target * local_experts + j]

    def relay(c, source, s):
        w, j = blocks[c]
        return relays[w].at[j, source, s]

    def tp_copy(c, d, s, to_out):
        target = lax.rem(t + d, tp)
        return pltpu.make_async_remote_copy(
            src_ref=own(c, target, s),
            dst_ref=out_rows(c, g, f) if to_out else relay(c, t, s),
            send_sem=tp_send.at[c, d, s],
            recv_sem=tp_recv.at[c, d, s],
            device_id={"tp": target},
            device_id_type=MESH,
        )

    def fs_copy(c, d, s, src, target):
        return pltpu.make_async_remote_copy(
            src_ref=src,
            dst_ref=out_rows(c, g, f),
            send_sem=fs_send.at[c, d, s],
            recv_sem=fs_recv.at[c, f],
            device_id={"fs": target},
            device_id_type=MESH,
        )

    def gr_copy(c, n, source, src):
        return pltpu.make_async_remote_copy(
            src_ref=src,
            dst_ref=out_rows(c, g, source),
            send_sem=gr_send.at[c, n, source],
            recv_sem=gr_recv.at[c, n, source],
            device_id={"gr": lax.rem(g + n, gr)},
            device_id_type=MESH,
        )

    def to_groups(c, source, src):
        for n in range(1, gr):
            gr_copy(c, n, source, src).start()

    def tp_start(c):
        for d in range(1, tp):
            for s in range(sub):

                @pl.when(t * sub + s == f)
                def _():
                    tp_copy(c, d, s, True).start()

                @pl.when(t * sub + s != f)
                def _():
                    tp_copy(c, d, s, False).start()

    def own_start(c):
        for s in range(sub):
            target = t * sub + s

            @pl.when(target != f)
            def _():
                fs_copy(c, 0, s, own(c, t, s), target).start()

            @pl.when(target == f)
            def _():
                pltpu.make_async_copy(own(c, t, s), bounce.at[c], load_sem.at[c]).start()
                to_groups(c, f, own(c, t, s))

    def own_store(c):
        for s in range(sub):

            @pl.when(t * sub + s == f)
            def _():
                pltpu.make_async_copy(own(c, t, s), bounce.at[c], load_sem.at[c]).wait()
                pltpu.make_async_copy(bounce.at[c], out_rows(c, g, f), store_sem.at[c]).start()

    def tp_arrived(c):
        for d in range(1, tp):
            source = lax.rem(t + tp - d, tp)
            for s in range(sub):
                target = source * sub + s

                @pl.when(target == f)
                def _():
                    tp_copy(c, d, s, True).wait_recv()
                    to_groups(c, f, out_rows(c, g, f))

                @pl.when(target != f)
                def _():
                    pltpu.make_async_remote_copy(
                        src_ref=own(c, t, s),
                        dst_ref=relay(c, source, s),
                        send_sem=tp_send.at[c, d, s],
                        recv_sem=tp_recv.at[c, d, s],
                        device_id={"tp": source},
                        device_id_type=MESH,
                    ).wait_recv()
                    fs_copy(c, d, s, relay(c, source, s), target).start()

    def fs_arrived(c):
        for d in range(1, fs):
            source = lax.rem(f + d, fs)
            pltpu.make_async_remote_copy(
                src_ref=own(c, t, 0),
                dst_ref=out_rows(c, g, source),
                send_sem=fs_send.at[c, 0, 0],
                recv_sem=fs_recv.at[c, source],
                device_id={"fs": source},
                device_id_type=MESH,
            ).wait_recv()
            to_groups(c, source, out_rows(c, g, source))

    total = len(blocks)
    ahead = min(3, total)
    own_start(0)
    for c in range(ahead):
        tp_start(c)
    for c in range(total + 1):
        if c + ahead < total:
            tp_start(c + ahead)
        if c + 1 < total:
            own_start(c + 1)
        if c < total:
            own_store(c)
            tp_arrived(c)
        if c >= 1:
            fs_arrived(c - 1)

    for c in range(total):
        for n in range(1, gr):
            for source in range(fs):
                group = lax.rem(g + gr - n, gr)
                pltpu.make_async_remote_copy(
                    src_ref=own(c, t, 0),
                    dst_ref=out_rows(c, group, source),
                    send_sem=gr_send.at[c, n, source],
                    recv_sem=gr_recv.at[c, n, source],
                    device_id={"gr": group},
                    device_id_type=MESH,
                ).wait_recv()
                gr_copy(c, n, source, out_rows(c, g, source)).wait_send()
        for s in range(sub):
            for d in range(1, tp):
                tp_copy(c, d, s, False).wait_send()
            for d in range(tp):
                target = lax.rem(t + tp - d, tp) * sub + s

                @pl.when(target != f)
                def _():
                    fs_copy(c, d, s, own(c, t, s), target).wait_send()

            @pl.when(t * sub + s == f)
            def _():
                pltpu.make_async_copy(bounce.at[c], out_rows(c, g, f), store_sem.at[c]).wait()


def spread(*weights):
    gr, fs, tp = lax.axis_size("gr"), lax.axis_size("fs"), lax.axis_size("tp")
    experts, rows, columns = weights[0].shape
    local_experts = experts // tp
    assert fs % tp == 0
    sub = fs // tp
    width = columns // sub
    count = len(weights)
    total = count * local_experts
    flipped = rows % 128 == 0
    order = (2, 0, 3, 1) if flipped else (2, 0, 1, 3)
    parts = [w.reshape(experts, rows, sub, width).transpose(order) for w in weights]
    block = (width, rows) if flipped else (rows, width)
    whole = (width, gr * fs * rows) if flipped else (gr * fs * rows, width)
    served = jax.ShapeDtypeStruct((local_experts, *whole), jnp.bfloat16)
    relayed = jax.ShapeDtypeStruct((local_experts, tp, sub, *block), jnp.bfloat16)
    dma = pltpu.SemaphoreType.DMA
    sent = 2 * total * rows * columns * (tp - 1 + fs - 1 + (gr - 1) * fs) // fs
    found = pl.pallas_call(
        functools.partial(spread_kernel, (gr, fs, tp, sub, local_experts, rows), count, flipped),
        out_shape=[served] * count + [relayed] * count,
        in_specs=[pl.BlockSpec(memory_space=pl.ANY)] * count,
        out_specs=[pl.BlockSpec(memory_space=pl.ANY)] * (2 * count),
        scratch_shapes=[
            pltpu.VMEM((total, *block), jnp.bfloat16),
            dma((total, tp, sub)),
            dma((total, tp, sub)),
            dma((total, tp, sub)),
            dma((total, fs)),
            dma((total, gr, fs)),
            dma((total, gr, fs)),
            dma((total,)),
            dma((total,)),
        ],
        compiler_params=pltpu.CompilerParams(collective_id=0, has_side_effects=True),
        cost_estimate=pl.CostEstimate(flops=0, bytes_accessed=40 * sent, transcendentals=0),
    )(*parts)
    return [w.swapaxes(1, 2) if flipped else w for w in found[:count]]


def local_by_collectives(tokens, routes, route_weight, norm_gain, gate_master, up_master, down_master):
    experts = gate_master.shape[0]
    tp_count = lax.axis_size("tp")
    fs_count = lax.axis_size("fs")
    local_experts = experts // tp_count
    token_rows = tokens.shape[0]
    model_width = tokens.shape[1] * fs_count
    capacity = 3 * token_rows // experts
    scaled_gain = norm_gain[None, :, None]
    gate_w = (gate_master * scaled_gain).astype(jnp.bfloat16)
    up_w = (up_master * scaled_gain).astype(jnp.bfloat16)
    down_w = down_master.astype(jnp.bfloat16)
    gate_w, up_w, down_w = spread(gate_w, up_w, down_w)
    as_float = tokens.astype(jnp.float32)
    square_total = lax.psum(jnp.sum(as_float * as_float, axis=1), "fs")
    normed = (as_float * lax.rsqrt(square_total / model_width + norm_eps)[:, None]).astype(
        jnp.bfloat16
    )
    placing = slot_table(routes, experts, capacity)
    slot_rows = jnp.arange(experts * capacity, dtype=jnp.int32)
    picked = (slot_rows[:, None] == placing[None, :]).reshape(experts * capacity, token_rows, 2)
    route_table = jnp.sum(picked.astype(jnp.float32), axis=2).astype(jnp.bfloat16)
    outgoing = jnp.dot(route_table, normed, preferred_element_type=jnp.float32).astype(jnp.bfloat16)
    outgoing = outgoing.reshape(tp_count, local_experts, capacity, tokens.shape[1])
    shard_piece = lax.all_gather(
        lax.all_to_all(outgoing, "tp", split_axis=0, concat_axis=0, tiled=True),
        "fs",
        axis=3,
        tiled=True,
    )
    returned = []
    for j in range(local_experts):
        rows = shard_piece[:, j]
        gate_acc = jnp.einsum("scd,df->scf", rows, gate_w[j], preferred_element_type=jnp.float32)
        up_acc = jnp.einsum("scd,df->scf", rows, up_w[j], preferred_element_type=jnp.float32)
        hidden = (jax.nn.silu(gate_acc) * up_acc).astype(jnp.bfloat16)
        partial_value = jnp.einsum(
            "scf,df->scd", hidden, down_w[j], preferred_element_type=jnp.float32
        )
        summed = lax.psum_scatter(
            partial_value.astype(jnp.bfloat16), "fs", scatter_dimension=2, tiled=True
        )
        returned.append(lax.all_to_all(summed, "tp", split_axis=0, concat_axis=0, tiled=True))
    produced = jnp.stack(returned, axis=1)
    produced = produced.reshape(experts * capacity, produced.shape[3])
    pair_slots = placing.reshape(token_rows, 2)
    first_rows = jnp.take(produced, pair_slots[:, 0], axis=0)
    second_rows = jnp.take(produced, pair_slots[:, 1], axis=0)
    mixed_out = first_rows * route_weight[:, 0:1] + second_rows * route_weight[:, 1:2]
    return (mixed_out.astype(jnp.bfloat16), gate_w, up_w, down_w)


def slot_places(routes, experts, capacity):
    rows = routes.shape[0]
    hits = (routes[:, :, None] == jnp.arange(experts, dtype=jnp.int32)).astype(jnp.int32)
    both = hits[:, 0] + hits[:, 1]
    before = jnp.cumsum(both, axis=0) - both
    first = jnp.sum(hits[:, 0] * before, axis=1)
    second = jnp.sum(hits[:, 1] * (before + hits[:, 0]), axis=1)
    places = jnp.stack([first, second]) + routes.T * capacity
    return jnp.pad(places, ((0, 6), (0, 0)))


def serve_kernel(sizes, *refs):
    gr, fs, tp, local_experts, rows, capacity = sizes
    tokens, places, shares = refs[:3]
    ins, outs, relays, mixed = refs[3:6], refs[6:9], refs[9:12], refs[12]
    (
        bounce_in, bounce_down, gathered, place_of, share_of, picks, slot_share, slots, hid, spread_hid,
        gate_buf, up_buf, down_buf, part, from_core, to_side, from_side, to_fs, from_near,
        from_far, kept, kept_far, mixed_buf,
        tp_send, tp_recv, fs_send, fs_recv, gr_send, gr_recv, load_sem, store_sem,
        up_sem, low_sem, slab_recv, core_send, side_send, block_recv, info_send, info_recv,
        own_sem, weight_sem, down_sem, core_psend, core_precv, side_psend, side_precv,
        near_send, near_recv, far_send, far_recv, mixed_sem,
    ) = refs[13:]
    g, f, t = lax.axis_index("gr"), lax.axis_index("fs"), lax.axis_index("tp")
    bounce = (bounce_in, bounce_down)
    halves = 2
    half = rows // halves
    blocks = [(w, j) for j in range(local_experts) for w in range(2)]
    blocks += [(2, h) for h in range(halves)]
    total = len(blocks)
    token_rows, features = tokens.shape
    width = fs * features

    barrier = pltpu.get_barrier_semaphore()
    for axis, me, size in (("gr", g, gr), ("fs", f, fs), ("tp", t, tp)):
        for d in range(1, size):
            pl.semaphore_signal(
                barrier, inc=1, device_id={axis: lax.rem(me + d, size)}, device_id_type=MESH
            )
    pl.semaphore_wait(barrier, gr + fs + tp - 3)

    def remote(src, dst, send, recv, axis, target):
        return pltpu.make_async_remote_copy(
            src_ref=src, dst_ref=dst, send_sem=send, recv_sem=recv,
            device_id={axis: target}, device_id_type=MESH,
        )

    def slab(block, source):
        return gathered.at[block, source]

    core = t + 1 - 2 * lax.rem(t, 2)
    side = lax.rem(t + 2, tp)
    core_side = lax.rem(core + 2, tp)

    def slab_copy(source, up):
        mine = slab(t, source)
        sem = (up_sem if up else low_sem).at[source]
        return remote(mine, mine, sem, slab_recv.at[source], "fs", f + 1 if up else f - 1)

    def slab_pass(source, up):
        @pl.when(f < fs - 1 if up else f > 0)
        def _():
            slab_copy(source, up).start()

    def to_core(k, source):
        mine = slab((t, side)[k], source)
        return remote(
            mine, mine, core_send.at[k, source], block_recv.at[(t, side)[k], source], "tp", core
        )

    def to_sides(source):
        mine = slab(t, source)
        return remote(
            mine, mine, side_send.at[source], block_recv.at[t, source], "tp", side
        )

    def slab_spread(source):
        to_sides(source).start()
        to_core(0, source).start()

    def slab_arrived(k):
        for up in (True, False):
            source = f - k if up else f + k

            @pl.when(source >= 0 if up else source < fs)
            def _():
                slab_copy(source, up).wait_recv()
                slab_pass(source, up)
                slab_spread(source)

    def block_wait(block, source):
        mine = slab(block, source)
        remote(
            mine, mine, side_send.at[source], block_recv.at[block, source], "tp", side
        ).wait_recv()

    def side_arrived(k):
        source = lax.rem(f + k, fs)
        block_wait(side, source)
        to_core(1, source).start()

    def core_arrived():
        for block in (core, core_side):
            for source in range(fs):
                block_wait(block, source)
        for d in range(1, tp):
            source = lax.rem(t + d, tp)
            for k in range(2):
                whole = (place_of, share_of)[k]
                remote(
                    (places, shares)[k], whole.at[source], info_send.at[d, k],
                    info_recv.at[source, k], "tp", source,
                ).wait_recv()

    def info(d, k):
        whole = (place_of, share_of)[k]
        return remote(
            (places, shares)[k], whole.at[t], info_send.at[d, k], info_recv.at[t, k],
            "tp", lax.rem(t + d, tp),
        )

    def own_copies():
        return (
            pltpu.make_async_copy(tokens, slab(t, f), own_sem.at[0]),
            pltpu.make_async_copy(places, place_of.at[t], own_sem.at[1]),
            pltpu.make_async_copy(shares, share_of.at[t], own_sem.at[2]),
        )

    def out_rows(c, group, source):
        w, j = blocks[c]
        start = pl.multiple_of((group * fs + source) * rows, rows)
        if w == 2:
            return outs[w].at[:, :, pl.ds(start + j * half, half)]
        return outs[w].at[j, :, pl.ds(start, rows)]

    def own(c, target):
        w, j = blocks[c]
        if w == 2:
            first = target * local_experts
            return ins[w].at[pl.ds(first, local_experts), :, j * half : (j + 1) * half]
        return ins[w].at[target * local_experts + j]

    def relay(c, source):
        w, j = blocks[c]
        if w == 2:
            return relays[w].at[source, :, :, j * half : (j + 1) * half]
        return relays[w].at[j, source]

    def tp_copy(c, d, to_out):
        target = lax.rem(t + d, tp)
        return remote(
            own(c, target), out_rows(c, g, f) if to_out else relay(c, t),
            tp_send.at[c, d], tp_recv.at[c, d], "tp", target,
        )

    def fs_copy(c, d, src, target):
        return remote(src, out_rows(c, g, f), fs_send.at[c, d], fs_recv.at[c, f], "fs", target)

    def gr_copy(c, n, source, src):
        return remote(
            src, out_rows(c, g, source), gr_send.at[c, n, source], gr_recv.at[c, n, source],
            "gr", lax.rem(g + n, gr),
        )

    def to_groups(c, source, src):
        for n in range(1, gr):
            gr_copy(c, n, source, src).start()

    def tp_start(c):
        for d in range(1, tp):

            @pl.when(t == f)
            def _():
                tp_copy(c, d, True).start()

            @pl.when(t != f)
            def _():
                tp_copy(c, d, False).start()

    def bounce_of(c):
        w, j = blocks[c]
        return bounce[1].at[j] if w == 2 else bounce[0].at[c]

    def own_store(c):
        @pl.when(t == f)
        def _():
            pltpu.make_async_copy(own(c, t), bounce_of(c), load_sem.at[c]).wait()
            pltpu.make_async_copy(bounce_of(c), out_rows(c, g, f), store_sem.at[c]).start()

    def fs_send_next(c, k):
        odd = lax.rem(f, 2)
        source = lax.rem(f + (2, 3 - 2 * odd, 1 + 2 * odd)[k], fs)
        d = lax.rem(t - source + tp, tp)

        @pl.when(source == t)
        def _():
            fs_copy(c, d, own(c, t), source).start()

        @pl.when(source != t)
        def _():
            remote(
                own(c, t), relay(c, source), tp_send.at[c, d], tp_recv.at[c, d], "tp", source
            ).wait_recv()
            fs_copy(c, d, relay(c, source), source).start()

    def home(c):
        d = lax.rem(t - f + tp, tp)

        @pl.when(t == f)
        def _():
            pltpu.make_async_copy(own(c, t), bounce_of(c), load_sem.at[c]).start()
            to_groups(c, f, own(c, t))

        @pl.when(t != f)
        def _():
            tp_copy(c, d, True).wait_recv()
            to_groups(c, f, out_rows(c, g, f))

    def fs_arrived(c, k):
        odd = lax.rem(f, 2)
        source = lax.rem(f + (2, 3 - 2 * odd, 1 + 2 * odd)[k], fs)
        remote(
            own(c, t), out_rows(c, g, source), fs_send.at[c, 0], fs_recv.at[c, source],
            "fs", source,
        ).wait_recv()
        to_groups(c, source, out_rows(c, g, source))

    def gr_arrived(c):
        for n in range(1, gr):
            for source in range(fs):
                group = lax.rem(g + gr - n, gr)
                remote(
                    own(c, t), out_rows(c, group, source), gr_send.at[c, n, source],
                    gr_recv.at[c, n, source], "gr", group,
                ).wait_recv()

    def own_stored(c):
        @pl.when(t == f)
        def _():
            pltpu.make_async_copy(bounce_of(c), out_rows(c, g, f), store_sem.at[c]).wait()

    def sent(c):
        for n in range(1, gr):
            for source in range(fs):
                gr_copy(c, n, source, out_rows(c, g, source)).wait_send()
        for d in range(1, tp):
            tp_copy(c, d, False).wait_send()
        for d in range(tp):
            target = lax.rem(t + tp - d, tp)

            @pl.when(target != f)
            def _():
                fs_copy(c, d, own(c, t), target).wait_send()

    def pick_slots(j):
        @pl.loop(0, tp)
        def _(b):
            base = (t * local_experts + j) * capacity
            index = lax.broadcasted_iota(jnp.int32, (capacity, token_rows), 0) + base
            first = place_of[b, 0:1, :] == index
            second = place_of[b, 1:2, :] == index
            share = jnp.where(first, share_of[b, 0:1, :], 0.0)
            share = share + jnp.where(second, share_of[b, 1:2, :], 0.0)
            share = jnp.sum(share, axis=1, keepdims=True)
            at = pl.ds(pl.multiple_of(b * capacity, capacity), capacity)
            slot_share[at, :] = jnp.broadcast_to(share, (capacity, 128))
            pick = jnp.where(first | second, 1.0, 0.0).astype(jnp.bfloat16)
            picks[b] = pick
            squares = jnp.zeros((capacity, 1), jnp.float32)
            for q in range(fs):
                columns = slice(q * features, (q + 1) * features)
                raw = jnp.dot(
                    pick, gathered[b, q], preferred_element_type=jnp.float32
                )
                slots[at, columns] = raw.astype(jnp.bfloat16)
                squares = squares + jnp.sum(raw * raw, axis=1, keepdims=True)
            scale = lax.rsqrt(squares / width + norm_eps)
            for q in range(fs):
                columns = slice(q * features, (q + 1) * features)
                raw = slots[at, columns].astype(jnp.float32)
                slots[at, columns] = (raw * scale).astype(jnp.bfloat16)

    def weight_load(w, j):
        return pltpu.make_async_copy(outs[w].at[j], (gate_buf, up_buf)[w], weight_sem.at[w])

    def hidden_of(j, start):
        units = gate_buf.shape[0]
        step = 2 * capacity
        cut = slice(start, min(start + 256, units))

        @pl.loop(0, tp * capacity // step)
        def _(m):
            at = pl.ds(pl.multiple_of(m * step, step), step)
            into = (((1,), (1,)), ((), ()))
            gate = lax.dot_general(
                slots[at, :], gate_buf[cut, :], into, preferred_element_type=jnp.float32
            )
            up = lax.dot_general(
                slots[at, :], up_buf[cut, :], into, preferred_element_type=jnp.float32
            )
            value = gate / (1.0 + jnp.exp(-gate)) * up
            hid[at, cut] = (value * slot_share[at, 0:1]).astype(jnp.bfloat16)

    def hidden_to_tokens(j):
        @pl.loop(0, tp)
        def _(b):
            at = pl.ds(pl.multiple_of(b * capacity, capacity), capacity)
            spread_hid[j, b] = lax.dot_general(
                picks[b], hid[at, :], (((0,), (0,)), ((), ())),
                preferred_element_type=jnp.float32,
            ).astype(jnp.bfloat16)

    pieces = [(h, n) for h in range(halves) for n in range(fs)]
    upper = f // 2
    near = f + 1 - 2 * lax.rem(f, 2)
    inner = (f == 1) | (f == 2)

    def column_owner(n):
        return (3 - 3 * upper, 2 - upper, near, f)[n]

    joined = features // rows
    cut = joined * half

    def down_loads(p):
        h, n = pieces[p]
        q = column_owner(n)
        copies = []
        for i in range(joined):
            start = pl.multiple_of((q * joined + i) * rows, rows)
            copies.append(
                pltpu.make_async_copy(
                    outs[2].at[:, :, pl.ds(start + h * half, half)],
                    down_buf.at[p % 2, :, :, i * half : (i + 1) * half],
                    down_sem.at[p % 2, i],
                )
            )
        return copies

    def core_part(p, k):
        block = (core, core_side)[k]
        return remote(
            part.at[p, block], from_core.at[p, k], core_psend.at[p, k], core_precv.at[p, k],
            "tp", core,
        )

    def side_part(p):
        return remote(
            to_side.at[p], from_side.at[p], side_psend.at[p], side_precv.at[p], "tp", side
        )

    def near_part(p):
        return remote(to_fs.at[p], from_near.at[p], near_send.at[p], near_recv.at[p], "fs", near)

    def far_part(p):
        h, n = pieces[p]
        return remote(
            to_fs.at[p], from_far.at[h], far_send.at[p], far_recv.at[h], "fs", column_owner(n)
        )

    def piece_start(p):
        for copy in down_loads(p):
            copy.wait()
        if p + 1 < len(pieces) and pieces[p + 1][0] == pieces[p][0]:
            for copy in down_loads(p + 1):
                copy.start()

        @pl.loop(0, tp)
        def _(b):
            value = jnp.dot(
                spread_hid[0, b], down_buf[p % 2, 0], preferred_element_type=jnp.float32
            )
            for j in range(1, local_experts):
                value = value + jnp.dot(
                    spread_hid[j, b], down_buf[p % 2, j], preferred_element_type=jnp.float32
                )
            part[p, b] = value.astype(jnp.bfloat16)

        for k in range(2):
            core_part(p, k).start()

    def piece_side(p):
        for k in range(2):
            core_part(p, k).wait_recv()
        value = part[p, side].astype(jnp.float32) + from_core[p, 1].astype(jnp.float32)
        to_side[p] = value.astype(jnp.bfloat16)
        side_part(p).start()

    def piece_fs(p):
        h, n = pieces[p]
        side_part(p).wait_recv()
        value = part[p, t].astype(jnp.float32) + from_core[p, 0].astype(jnp.float32)
        value = value + from_side[p].astype(jnp.float32)
        if n == 3:
            kept[h] = value
        elif n == 2:
            to_fs[p] = value.astype(jnp.bfloat16)
            near_part(p).start()
        else:
            @pl.when(inner)
            def _():
                kept_far[p % 2] = value

            @pl.when(jnp.logical_not(inner))
            def _():
                to_fs[p] = value.astype(jnp.bfloat16)
                near_part(p).start()

    def piece_far(p):
        h, n = pieces[p]

        @pl.when(inner)
        def _():
            near_part(p).wait_recv()
            value = kept_far[p % 2] + from_near[p].astype(jnp.float32)
            to_fs[p] = value.astype(jnp.bfloat16)
            far_part(p).start()

    def finish(h):
        value = kept[h]
        near_part(h * fs + 2).wait_recv()
        value = value + from_near[h * fs + 2].astype(jnp.float32)
        far_part(h * fs).wait_recv()
        value = value + from_far[h].astype(jnp.float32)
        value = value.astype(jnp.bfloat16)
        for i in range(joined):
            first = i * rows + h * half
            mixed_buf[:, first : first + half] = value[:, i * half : (i + 1) * half]

    def all_pieces(h):
        own_pieces = [p for p in range(len(pieces)) if pieces[p][0] == h]
        thunks = [lambda: [copy.start() for copy in down_loads(own_pieces[0])]]
        for n in range(len(own_pieces) + 2):
            if n < len(own_pieces):
                thunks.append(functools.partial(piece_start, own_pieces[n]))
            if 1 <= n <= len(own_pieces):
                thunks.append(functools.partial(piece_side, own_pieces[n - 1]))
            if n >= 2:
                thunks.append(functools.partial(piece_fs, own_pieces[n - 2]))
            if n in (3, 4):
                thunks.append(functools.partial(piece_far, own_pieces[n - 3]))
        return thunks

    def expert_thunks(j):
        def begin():
            for w in range(2):
                gr_arrived(2 * j + w)
                own_stored(2 * j + w)
                weight_load(w, j).start()
            pick_slots(j)
            weight_load(0, j).wait()
            weight_load(1, j).wait()

        units = gate_buf.shape[0]
        cuts = [functools.partial(hidden_of, j, start) for start in range(0, units, 256)]
        return [begin, *cuts, functools.partial(hidden_to_tokens, j)]

    own_load = own_copies()
    for copy in own_load:
        copy.start()
    for up in (True, False):
        @pl.when(f < fs - 1 if up else f > 0)
        def _():
            remote(
                tokens, slab(t, f), (up_sem if up else low_sem).at[f], slab_recv.at[f],
                "fs", f + 1 if up else f - 1,
            ).start()
    for d in range(1, tp):
        for k in range(2):
            info(d, k).start()
    early = min(4, total)
    for c in range(early):
        tp_start(c)
    own_load[0].wait()
    slab_spread(f)

    def out_waits(c):
        return [
            functools.partial(home, c),
            *[functools.partial(fs_send_next, c, k) for k in range(fs - 1)],
        ]

    def fs_waits(c):
        return [functools.partial(fs_arrived, c, k) for k in range(fs - 1)]

    def mix(waits, todo):
        for n, wait in enumerate(waits):
            wait()
            take = -(-len(todo) // (len(waits) - n))
            for thunk in todo[:take]:
                thunk()
            todo = todo[take:]
        for thunk in todo:
            thunk()

    def both(first, second):
        longer = max(len(first), len(second))
        found = []
        for n in range(longer):
            found += first[n : n + 1] + second[n : n + 1]
        return found

    mix(out_waits(0), [])
    slab_arrived(1)
    own_store(0)
    mix(out_waits(1), [])
    mix(fs_waits(0), [])
    slab_arrived(2)
    own_store(1)
    mix(out_waits(2), [])
    mix(fs_waits(1), [])
    slab_arrived(3)
    for c in range(early, total):
        tp_start(c)
    own_store(2)
    mix(out_waits(3), [])
    mix(fs_waits(2), [])
    own_load[1].wait()
    own_load[2].wait()
    sides = [functools.partial(side_arrived, k) for k in range(fs)]
    own_store(3)
    mix(out_waits(4), sides)
    mix(fs_waits(3), [])
    core_arrived()
    own_store(4)
    mix(out_waits(5), [])
    mix(fs_waits(4), expert_thunks(0))
    own_store(5)
    mix(fs_waits(5), expert_thunks(1))
    gr_arrived(4)
    own_stored(4)
    mix(all_pieces(0), [])
    for h in range(1, halves):
        c = 2 * local_experts + h
        gr_arrived(c)
        own_stored(c)
        for thunk in all_pieces(h):
            thunk()
    for h in range(halves):
        finish(h)
    store = pltpu.make_async_copy(mixed_buf, mixed, mixed_sem)
    store.start()

    for c in range(total):
        sent(c)
    for source in range(fs):
        for up in (True, False):
            @pl.when((f < fs - 1) & (source <= f) if up else (f > 0) & (source >= f))
            def _():
                slab_copy(source, up).wait_send()
        to_sides(source).wait_send()
        to_core(0, source).wait_send()
        to_core(1, source).wait_send()
    for d in range(1, tp):
        for k in range(2):
            info(d, k).wait_send()
    for p in range(len(pieces)):
        for k in range(2):
            core_part(p, k).wait_send()
        side_part(p).wait_send()
        if pieces[p][1] == 2:
            near_part(p).wait_send()
        elif pieces[p][1] < 2:
            @pl.when(inner)
            def _():
                far_part(p).wait_send()

            @pl.when(jnp.logical_not(inner))
            def _():
                near_part(p).wait_send()
    store.wait()


def serve(tokens, places, shares, capacity, *weights):
    gr, fs, tp = lax.axis_size("gr"), lax.axis_size("fs"), lax.axis_size("tp")
    experts, rows, columns = weights[0].shape
    local_experts = experts // tp
    token_rows, features = tokens.shape
    width = features * fs
    parts = [w.transpose(0, 2, 1) for w in weights]
    block = (columns, rows)
    bf16, f32 = jnp.bfloat16, jnp.float32
    served = jax.ShapeDtypeStruct((local_experts, columns, width), bf16)
    relayed = jax.ShapeDtypeStruct((local_experts, tp, *block), bf16)
    relayed_down = jax.ShapeDtypeStruct((tp, local_experts, *block), bf16)
    half, pieces = rows // 2, 2 * fs
    cut = features // rows * half
    total = 2 * local_experts + 2
    dma = pltpu.SemaphoreType.DMA
    anywhere = pl.BlockSpec(memory_space=pl.ANY)
    slots = tp * capacity
    found = pl.pallas_call(
        functools.partial(serve_kernel, (gr, fs, tp, local_experts, rows, capacity)),
        out_shape=[served] * 3
        + [relayed] * 2
        + [relayed_down, jax.ShapeDtypeStruct((token_rows, features), bf16)],
        in_specs=[anywhere] * 6,
        out_specs=[anywhere] * 7,
        scratch_shapes=[
            pltpu.VMEM((2 * local_experts, *block), bf16),
            pltpu.VMEM((2, local_experts, columns, half), bf16),
            pltpu.VMEM((tp, fs, token_rows, features), bf16),
            pltpu.VMEM((tp, *places.shape), jnp.int32),
            pltpu.VMEM((tp, *shares.shape), f32),
            pltpu.VMEM((tp, capacity, token_rows), bf16),
            pltpu.VMEM((slots, 128), f32),
            pltpu.VMEM((slots, width), bf16),
            pltpu.VMEM((slots, columns), bf16),
            pltpu.VMEM((local_experts, tp, token_rows, columns), bf16),
            pltpu.VMEM((columns, width), bf16),
            pltpu.VMEM((columns, width), bf16),
            pltpu.VMEM((2, local_experts, columns, cut), bf16),
            pltpu.VMEM((pieces, tp, token_rows, cut), bf16),
            pltpu.VMEM((pieces, 2, token_rows, cut), bf16),
            pltpu.VMEM((pieces, token_rows, cut), bf16),
            pltpu.VMEM((pieces, token_rows, cut), bf16),
            pltpu.VMEM((pieces, token_rows, cut), bf16),
            pltpu.VMEM((pieces, token_rows, cut), bf16),
            pltpu.VMEM((2, token_rows, cut), bf16),
            pltpu.VMEM((2, token_rows, cut), f32),
            pltpu.VMEM((2, token_rows, cut), f32),
            pltpu.VMEM((token_rows, features), bf16),
            dma((total, tp)),
            dma((total, tp)),
            dma((total, tp)),
            dma((total, fs)),
            dma((total, gr, fs)),
            dma((total, gr, fs)),
            dma((total,)),
            dma((total,)),
            dma((fs,)),
            dma((fs,)),
            dma((fs,)),
            dma((2, fs)),
            dma((fs,)),
            dma((tp, fs)),
            dma((tp, 2)),
            dma((tp, 2)),
            dma((3,)),
            dma((2,)),
            dma((2, features // rows)),
            dma((pieces, 2)),
            dma((pieces, 2)),
            dma((pieces,)),
            dma((pieces,)),
            dma((pieces,)),
            dma((pieces,)),
            dma((pieces,)),
            dma((2,)),
            dma,
        ],
        compiler_params=pltpu.CompilerParams(
            collective_id=0, has_side_effects=True, vmem_limit_bytes=60 * 1024 * 1024
        ),
        name="serve",
    )(tokens, places, shares, *parts)
    return [w.swapaxes(1, 2) for w in found[:3]], found[6]


def local(tokens, routes, route_weight, norm_gain, gate_master, up_master, down_master):
    experts, rows, columns = gate_master.shape
    gr, fs, tp = lax.axis_size("gr"), lax.axis_size("fs"), lax.axis_size("tp")
    token_rows, features = tokens.shape
    capacity = 3 * token_rows // experts
    fits = fs == tp and rows % 128 == 0 and features % 128 == 0 and features % rows == 0
    if not (fits and tp == 4 and rows % 256 == 0 and capacity % 16 == 0 and columns % 16 == 0):
        return local_by_collectives(
            tokens, routes, route_weight, norm_gain, gate_master, up_master, down_master
        )
    scaled_gain = norm_gain[None, :, None]
    gate_w = (gate_master * scaled_gain).astype(jnp.bfloat16)
    up_w = (up_master * scaled_gain).astype(jnp.bfloat16)
    down_w = down_master.astype(jnp.bfloat16)
    places = slot_places(routes, experts, capacity)
    shares = jnp.pad(route_weight.T, ((0, 6), (0, 0)))
    served, mixed = serve(tokens, places, shares, capacity, gate_w, up_w, down_w)
    return (mixed, *served)


def solution(mesh):
    placed = (
        P(("gr", "tp"), "fs"),
        P(("gr", "tp"), None),
        P(("gr", "tp"), None),
        P(("gr", "fs")),
        P(None, ("gr", "fs"), "tp"),
        P(None, ("gr", "fs"), "tp"),
        P(None, ("gr", "fs"), "tp"),
    )
    return jax.shard_map(
        local,
        mesh=mesh,
        in_specs=placed,
        out_specs=(
            P(("gr", "tp"), "fs"),
            P("tp", None, "fs"),
            P("tp", None, "fs"),
            P("tp", None, "fs"),
        ),
        check_vma=False,
    )
```
